256 devices in a mesh: grp: 2 (over y), sp: 32 (over z, core), tp: 4 (over x).
Axes of the slice: x: 4, y: 2, z: 16, core: 2. Of those that a mesh axis runs over, the one named last changes fastest.
The devices are a block of a 4x16x16 slice.
Arguments:
- residual_in: bfloat16 [16384, 2048], P(('grp', 'sp', 'tp')), parts along dimension 0, may hold values from -6 to 6
- q_small: bfloat16 [16384, 1024], P(('grp', 'sp'), 'tp'), parts along dimension 0, may hold values from -5 to 5
- k_small: bfloat16 [16384, 256], P(('grp', 'sp'), 'tp'), parts along dimension 0, may hold values from -5 to 5
- v_small: bfloat16 [16384, 256], P(('grp', 'sp'), 'tp'), parts along dimension 0, may hold values from -6 to 6
- q_large: bfloat16 [16384, 1024], P(('grp', 'sp'), 'tp'), parts along dimension 0, may hold values from -5 to 5
- k_large: bfloat16 [16384, 512], P(('grp', 'sp'), 'tp'), parts along dimension 0, may hold values from -5 to 5
- v_large: bfloat16 [16384, 512], P(('grp', 'sp'), 'tp'), parts along dimension 0, may hold values from -6 to 6
- gain_qs: float32 [64], replicated, may hold values from 0.24 to 7.4
- gain_ks: float32 [64], replicated, may hold values from 0.24 to 7.4
- gain_ql: float32 [128], replicated, may hold values from 0.24 to 7.4
- gain_kl: float32 [128], replicated, may hold values from 0.24 to 7.4
- w_out_small: bfloat16 [1024, 2048], P('tp'), may hold values from -0.125 to 0.125
- w_out_large: bfloat16 [1024, 2048], P('tp'), may hold values from -0.125 to 0.125
- g_ffn: float32 [2048], replicated, may hold values from 0.1 to 1.9
- routes: int32 [16384, 4], P(('grp', 'sp', 'tp')), parts along dimension 0, may hold values from 0 to 63, all different within a row; in each aligned block of 64 rows (0 to 63, 64 to 127, ...) at most 8 rows name the same one
- route_w: float32 [16384, 4], P(('grp', 'sp', 'tp')), parts along dimension 0, may hold values from 0.2 to 1
- w_gate: bfloat16 [64, 2048, 1024], P('sp', None, 'tp'), may hold values from -0.125 to 0.125
- w_up: bfloat16 [64, 2048, 1024], P('sp', None, 'tp'), may hold values from -0.125 to 0.125
- w_down: bfloat16 [64, 1024, 2048], P('sp', 'tp'), may hold values from -0.1875 to 0.1875
- ws_gate: bfloat16 [2048, 1024], P(None, 'tp'), may hold values from -0.125 to 0.125
- ws_up: bfloat16 [2048, 1024], P(None, 'tp'), may hold values from -0.125 to 0.125
- ws_down: bfloat16 [1024, 2048], P('tp'), may hold values from -0.1875 to 0.1875
Outputs:
- result: bfloat16 [16384, 2048], P(('grp', 'sp', 'tp')), parts along dimension 0
The draws below stay inside these ranges and needn't reach their ends.
There are 2 independent parts, one for each index of `grp`. The reference program is written for one: setup_inputs(seed, part) draws one part's arguments, and reference() takes and returns one part's arrays. A program takes and returns all parts, laid end to end along the dimension named above; an argument that names none is the same for every part. Nothing has to cross between parts.
Inputs may be any that keep to these rules, and one draw needn't show every extreme that they name: `routes`: each row names 4 different experts. Among the rows of one device no expert is named more than 8 times, a bound that some block reaches.
All inputs are finite; a program needn't handle non-finite values.
Results may differ from the reference program's by a relative error of at most 0.018.
The reference program's roundings to bfloat16 on the way count: a program that leaves them out, or rounds other values in their place, can miss the bound.
Values may be sent and summed in bfloat16 or wider, within the bound.
A program may use at most 128 MiB of HBM per device.

```python
import math
import jax
import jax.numpy as jnp
import numpy as np
from jax import lax

D = 2048
QA = 16
HS_SMALL = 64
KVA = 4
QB = 8
HS_LARGE = 128
KVB = 4
FF = 1024
FF_SH = 1024
GRID_W = 64
TOPK = 4
TOKENS = 8192
ROWS_DEV = 64
EXPERTS = 64
CAP = 8
N_SP = 32
N_TP = 4


def paired_heads(key, kv_heads, head_width, query_heads):
    key_rows = jax.random.normal(jax.random.fold_in(key, 701 + head_width), (TOKENS, kv_heads, head_width), jnp.float32)
    queries = jax.random.normal(jax.random.fold_in(key, 702 + head_width), (TOKENS, kv_heads, query_heads // kv_heads, head_width), jnp.float32)
    queries = jnp.clip(queries, -5.0, 5.0)
    key_rows = jnp.clip(key_rows, -5.0, 5.0)
    return (queries.reshape(TOKENS, query_heads * head_width), key_rows.reshape(TOKENS, kv_heads * head_width))


def positive_gain(key, channels, salt):
    return jnp.exp(jax.random.uniform(jax.random.fold_in(key, salt), (channels,), jnp.float32, -1.4, 1.4))


def draw_q_small(key, part):
    return paired_heads(key, KVA, HS_SMALL, QA)[0].astype(jnp.bfloat16)


def draw_k_small(key, part):
    return paired_heads(key, KVA, HS_SMALL, QA)[1].astype(jnp.bfloat16)


def draw_q_large(key, part):
    return paired_heads(key, KVB, HS_LARGE, QB)[0].astype(jnp.bfloat16)


def draw_k_large(key, part):
    return paired_heads(key, KVB, HS_LARGE, QB)[1].astype(jnp.bfloat16)


def draw_gain_qs(key, part):
    return positive_gain(key, HS_SMALL, 811)


def draw_gain_ks(key, part):
    return positive_gain(key, HS_SMALL, 812)


def draw_gain_ql(key, part):
    return positive_gain(key, HS_LARGE, 813)


def draw_gain_kl(key, part):
    return positive_gain(key, HS_LARGE, 814)


def levels(key, shape, shards, low, top_value):
    loudness, own = 1.0, jax.random.fold_in(key, 6)
    for dim, shards_of in shards:
        heights = jnp.exp(jax.random.uniform(jax.random.fold_in(own, dim), (shards_of,), jnp.float32, low / len(shards), top_value / len(shards)))
        loudness = loudness * jnp.repeat(heights, shape[dim] // shards_of).reshape([-1 if axis == dim else 1 for axis in range(len(shape))])
    return loudness


def deal_out(key, own, number, rows, amount, top, bound, skew):
    sequence = jax.random.permutation(key, amount)
    heavy_load, usual = load_shares(amount, rows * top, bound, skew, True), load_shares(amount, rows * top, bound, skew, False)
    places = jnp.arange(amount)

    def named(tallies, turn):
        used = int((tallies > 0).sum())
        fixed = max(1, used // 4)
        moved = fixed + (places - fixed + turn * (used - fixed)) % max(1, amount - fixed)
        return jnp.zeros((amount,), jnp.int32).at[sequence[jnp.where(places < fixed, places, moved)]].set(jnp.asarray(tallies, jnp.int32))

    tallies = jnp.where(number % 4 == 0, named(heavy_load, number // 4), named(usual, number - number // 4 - 1))
    mixed = jax.random.permutation(jax.random.fold_in(own, 3), amount)
    giver, taker = mixed[0:amount // 2 * 2:2], mixed[1:amount // 2 * 2:2]
    margin = jnp.minimum(tallies[giver] - 1, bound - tallies[taker]) // 2
    margin = jnp.where((giver == sequence[0]) | (taker == sequence[0]) | (tallies[taker] == 0), 0, jnp.maximum(margin, 0))
    moved = jax.random.randint(jax.random.fold_in(own, 4), (amount // 2,), 0, 1 << 20) % (margin + 1)
    tallies = tallies.at[giver].add(-moved).at[taker].add(moved)
    items = jnp.searchsorted(jnp.cumsum(tallies), jnp.arange(rows * top), side="right").astype(jnp.int32)
    table = items.reshape(top, rows).T
    table = table[jax.random.permutation(jax.random.fold_in(own, 1), rows)]
    turn = jax.random.randint(jax.random.fold_in(own, 2), (rows, 1), 0, top)
    return jnp.take_along_axis(table, (jnp.arange(top)[None, :] + turn) % top, axis=1)


def load_shares(number_of, total, limit, skew, full):
    loads = [(1 << 20) // math.isqrt(rank ** skew) + 1 for rank in range(1, number_of + 1)]
    largest = limit if full else min(limit, max(-(-total // number_of), total * loads[0] // sum(loads)))
    least = 1 if total - largest >= number_of - 1 else 0
    holding, rest = [largest] + [least] * (number_of - 1), total - largest - least * (number_of - 1)
    while rest > 0:
        candidates = [i for i in range(1, number_of) if holding[i] < largest] or [i for i in range(1, number_of) if holding[i] < limit]
        pool, budget = sum([loads[i] for i in candidates]), rest
        for i in candidates:
            addition = min(limit - holding[i], max(1, budget * loads[i] // pool), rest)
            holding[i] = holding[i] + addition
            rest = rest - addition
    return np.array(holding)


def scatter_about(stream_key, shape, spread, bound, cuts=(), kind=jnp.bfloat16):
    level = levels(stream_key, shape, cuts, -0.22, 0.18) if cuts else 1.0
    entries = jax.random.normal(stream_key, shape, jnp.float32) * spread * level
    return jnp.minimum(jnp.maximum(entries, -bound), bound).astype(kind)


def setup_inputs(seed: int = 0, part: int = 0) -> dict:
    splits = jax.random.split(jax.random.key(seed), 23)
    part_keys = jax.random.split(jax.random.fold_in(splits[22], part), 23)
    residual_in = scatter_about(part_keys[0], (TOKENS, D), 1.0, 6.0, ((0, 128),))
    q_small = draw_q_small(jax.random.fold_in(jax.random.fold_in(splits[22], part), 71), part)
    k_small = draw_k_small(jax.random.fold_in(jax.random.fold_in(splits[22], part), 71), part)
    v_small = scatter_about(part_keys[3], (TOKENS, KVA * HS_SMALL), 1.0, 6.0, ((0, 32), (1, 4)))
    q_large = draw_q_large(jax.random.fold_in(jax.random.fold_in(splits[22], part), 71), part)
    k_large = draw_k_large(jax.random.fold_in(jax.random.fold_in(splits[22], part), 71), part)
    v_large = scatter_about(part_keys[6], (TOKENS, KVB * HS_LARGE), 1.0, 6.0, ((0, 32), (1, 4)))
    gain_qs = draw_gain_qs(jax.random.fold_in(splits[22], 71), part)
    gain_ks = draw_gain_ks(jax.random.fold_in(splits[22], 71), part)
    gain_ql = draw_gain_ql(jax.random.fold_in(splits[22], 71), part)
    gain_kl = draw_gain_kl(jax.random.fold_in(splits[22], 71), part)
    w_out_small = scatter_about(splits[11], (QA * HS_SMALL, D), (QA * HS_SMALL + QB * HS_LARGE) ** -0.5, 0.125, ((0, 4),))
    w_out_large = scatter_about(splits[12], (QB * HS_LARGE, D), (QA * HS_SMALL + QB * HS_LARGE) ** -0.5, 0.125, ((0, 4),))
    g_ffn = jnp.clip(1.0 + 0.18 * jax.random.normal(splits[13], (D,), jnp.float32), 0.1, 1.9)
    routes_keys = jax.random.split(jax.random.fold_in(part_keys[14], 1), TOKENS // ROWS_DEV)
    routes_turns = jax.random.permutation(jax.random.fold_in(part_keys[14], 3), TOKENS // ROWS_DEV)
    routes = jax.vmap(lambda own, number: deal_out(jax.random.fold_in(part_keys[14], 2), own, number, ROWS_DEV, EXPERTS, TOPK, CAP, 2))(routes_keys, routes_turns).reshape((TOKENS, TOPK))
    route_w = jnp.clip(0.2 + 0.8 * jax.random.uniform(part_keys[15], (TOKENS, TOPK), jnp.float32) ** levels(part_keys[15], (TOKENS, TOPK), ((0, 128),), -0.2, 0.2), 0.2, 1.0)
    w_gate = scatter_about(splits[16], (EXPERTS, D, FF), D ** -0.5, 0.125, ((0, 32), (2, 4)))
    w_up = scatter_about(splits[17], (EXPERTS, D, FF), D ** -0.5, 0.125, ((0, 32), (2, 4)))
    w_down = scatter_about(splits[18], (EXPERTS, FF, D), FF ** -0.5, 0.1875, ((0, 32), (1, 4)))
    ws_gate = scatter_about(splits[19], (D, FF_SH), D ** -0.5, 0.125, ((1, 4),))
    ws_up = scatter_about(splits[20], (D, FF_SH), D ** -0.5, 0.125, ((1, 4),))
    ws_down = scatter_about(splits[21], (FF_SH, D), FF_SH ** -0.5, 0.1875, ((0, 4),))
    return {"residual_in": residual_in, "q_small": q_small, "k_small": k_small, "v_small": v_small, "q_large": q_large, "k_large": k_large, "v_large": v_large, "gain_qs": gain_qs, "gain_ks": gain_ks, "gain_ql": gain_ql, "gain_kl": gain_kl, "w_out_small": w_out_small, "w_out_large": w_out_large, "g_ffn": g_ffn, "routes": routes, "route_w": route_w, "w_gate": w_gate, "w_up": w_up, "w_down": w_down, "ws_gate": ws_gate, "ws_up": ws_up, "ws_down": ws_down}


norm_eps = 1e-06
rope_base = 10000.0

def rounded(values):
    return lax.optimization_barrier(values.astype(jnp.bfloat16)).astype(jnp.float32)

def rotate_pairs(values, angles):
    front_half, back_half = jnp.split(values, 2, axis=-1)
    cosine_vals = jnp.cos(angles)[:, None, :]
    sine_vals = jnp.sin(angles)[:, None, :]
    return jnp.concatenate([front_half * cosine_vals - back_half * sine_vals, front_half * sine_vals + back_half * cosine_vals], axis=-1)

def norm_rotate(heads_in, gain, positions, grid_width):
    channels = gain.shape[0]
    values = heads_in.astype(jnp.float32).reshape(heads_in.shape[0], -1, channels)
    values = values * lax.rsqrt(lax.optimization_barrier(jnp.mean(values * values, axis=-1, keepdims=True)) + norm_eps) * gain
    quarter = channels // 4
    inverse = 1.0 / rope_base ** (jnp.arange(quarter, dtype=jnp.float32) / quarter)
    grid_rows = (positions // grid_width).astype(jnp.float32)
    grid_cols = (positions % grid_width).astype(jnp.float32)
    half_width = channels // 2
    turned = jnp.concatenate([rotate_pairs(values[..., :half_width], grid_rows[:, None] * inverse[None, :]), rotate_pairs(values[..., half_width:], grid_cols[:, None] * inverse[None, :])], axis=-1)
    return turned.astype(jnp.bfloat16)

def attend(queries, key_rows, value_rows):
    tokens, heads, channels = queries.shape
    kv_heads = key_rows.shape[1]
    group = heads // kv_heads
    block_rows = math.gcd(tokens, 256)
    blocks = queries.reshape(tokens // block_rows, block_rows, kv_heads, group, channels)
    keys32 = key_rows.astype(jnp.float32)
    values32 = value_rows.astype(jnp.float32)

    def one_block(query_block):
        scores = jnp.einsum('qkgd,skd->kgqs', query_block.astype(jnp.float32), keys32) * channels ** (-0.5)
        peak_val = lax.optimization_barrier(jnp.max(scores, axis=-1, keepdims=True))
        weights_raw = jnp.exp(scores - peak_val)
        totals = lax.optimization_barrier(jnp.sum(weights_raw, axis=-1))
        weights = rounded(weights_raw)
        mixture = jnp.einsum('kgqs,skd->qkgd', weights, values32)
        mixture = mixture / jnp.transpose(totals, (2, 0, 1))[..., None]
        return mixture.astype(jnp.bfloat16)
    result = lax.map(one_block, blocks)
    return result.reshape(tokens, heads * channels)

def split_down(hidden, down_w, pieces):
    columns = hidden.shape[1] // pieces
    summed = jnp.zeros((hidden.shape[0], down_w.shape[1]), jnp.float32)
    for device in range(pieces):
        term = jnp.dot(hidden[:, device * columns:(device + 1) * columns], down_w[device * columns:(device + 1) * columns], preferred_element_type=jnp.float32)
        summed = summed + rounded(term)
    return summed

def reference(residual_in, q_small, k_small, v_small, q_large, k_large, v_large, gain_qs, gain_ks, gain_ql, gain_kl, w_out_small, w_out_large, g_ffn, routes, route_w, w_gate, w_up, w_down, ws_gate, ws_up, ws_down):
    positions = jnp.arange(TOKENS, dtype=jnp.int32)
    heads_small = attend(norm_rotate(q_small, gain_qs, positions, GRID_W), norm_rotate(k_small, gain_ks, positions, GRID_W), v_small.reshape(TOKENS, KVA, HS_SMALL))
    heads_large = attend(norm_rotate(q_large, gain_ql, positions, GRID_W), norm_rotate(k_large, gain_kl, positions, GRID_W), v_large.reshape(TOKENS, KVB, HS_LARGE))
    small_cols = QA * HS_SMALL // N_TP
    large_cols = QB * HS_LARGE // N_TP
    head_sum = jnp.zeros((TOKENS, D), jnp.float32)
    for device in range(N_TP):
        term = jnp.dot(heads_small[:, device * small_cols:(device + 1) * small_cols], w_out_small[device * small_cols:(device + 1) * small_cols], preferred_element_type=jnp.float32)
        term = term + jnp.dot(heads_large[:, device * large_cols:(device + 1) * large_cols], w_out_large[device * large_cols:(device + 1) * large_cols], preferred_element_type=jnp.float32)
        head_sum = head_sum + rounded(term)
    stream32 = rounded(residual_in.astype(jnp.float32) + head_sum)
    normed = (stream32 * lax.rsqrt(lax.optimization_barrier(jnp.mean(stream32 * stream32, axis=-1, keepdims=True)) + norm_eps) * g_ffn).astype(jnp.bfloat16)
    assigned = TOKENS * TOPK
    flat_ids = routes.reshape(assigned)
    flat_weights = jnp.concatenate([route_w.reshape(assigned), jnp.zeros((1,), jnp.float32)])
    padded_rows = jnp.concatenate([normed, jnp.zeros((1, D), jnp.bfloat16)], axis=0)
    most_rows = N_SP * N_TP * CAP

    def one_expert(routed, inputs):
        expert, gate_w, up_w, down_w = inputs
        picked = jnp.nonzero(flat_ids == expert, size=most_rows, fill_value=assigned)[0].astype(jnp.int32)
        owners = jnp.where(picked < assigned, picked // TOPK, TOKENS).astype(jnp.int32)
        rows_in = padded_rows[owners]
        gate_act = jnp.dot(rows_in, gate_w, preferred_element_type=jnp.float32)
        up_act = jnp.dot(rows_in, up_w, preferred_element_type=jnp.float32)
        hidden = (jax.nn.silu(gate_act) * up_act).astype(jnp.bfloat16)
        expert_out = split_down(hidden, down_w, N_TP).astype(jnp.bfloat16)
        routed = routed.at[owners].add(flat_weights[picked][:, None] * expert_out.astype(jnp.float32))
        return (routed, None)
    routed, _ = lax.scan(one_expert, jnp.zeros((TOKENS + 1, D), jnp.float32), (jnp.arange(EXPERTS, dtype=jnp.int32), w_gate, w_up, w_down))
    shared_hidden = (jax.nn.silu(jnp.dot(normed, ws_gate, preferred_element_type=jnp.float32)) * jnp.dot(normed, ws_up, preferred_element_type=jnp.float32)).astype(jnp.bfloat16)
    shared = split_down(shared_hidden, ws_down, N_TP)
    return (stream32 + routed[:TOKENS] + shared).astype(jnp.bfloat16)
```

```python
import functools
import math

import jax
import jax.numpy as jnp
import numpy as np
from jax import lax
from jax.experimental import pallas as pl
from jax.experimental.pallas import tpu as pltpu
from jax.sharding import PartitionSpec as P

GRID_W = 64
TOPK = 4
norm_eps = 1e-06
rope_base = 10000.0
far_below = -1e30
LANES = 128
LOG2E = math.log2(math.e)
MESH = pl.DeviceIdType.MESH
F32 = jnp.float32
BF16 = jnp.bfloat16


def angle_tables(channels, rows_total):
    quarter = channels // 4
    lane = np.arange(LANES) % channels
    by_row = lane < channels // 2
    front = lane % (channels // 2) < quarter
    inverse = (1.0 / rope_base ** (np.arange(quarter, dtype=np.float32) / np.float32(quarter))).astype(np.float32)
    freq = inverse[lane % quarter]

    def tables(count, mask):
        angle = np.arange(count, dtype=np.float32)[:, None] * freq[None, :]
        angle = angle.astype(np.float32).astype(np.float64)
        cosine = np.where(mask[None, :], np.cos(angle), 0.0)
        sine = np.where(mask[None, :], np.where(front[None, :], -np.sin(angle), np.sin(angle)), 0.0)
        return cosine.astype(np.float32), sine.astype(np.float32)

    return tables(rows_total, by_row), tables(GRID_W, ~by_row)


def attention_kernel(
    chips, n_tp,
    q_s, k_s, v_s, q_l, k_l, v_l, g_qs, g_ks, g_ql, g_kl, row_tab, col_tab, w_s, w_l, resid, g_ffn,
    stream_out, normed_out,
    q_all, kv, m_ref, l_ref, acc, heads, part, got,
    rs, rr, ds, dr, xs, xr,
):
    me = lax.axis_index("sp")
    t = lax.axis_index("tp")
    z = me // 2
    c = me % 2
    rows = q_s.shape[0]
    half = rows // 2
    far = chips // 2
    tok = resid.shape[0]
    n_small = q_s.shape[1] // 64
    n_large = q_l.shape[1] // LANES

    def at(zz):
        return lax.rem(zz + 2 * chips, chips) * 2 + c

    right, left, mate = at(z + 1), at(z - 1), z * 2 + (1 - c)

    barrier = pltpu.get_barrier_semaphore()
    for peer in (right, left, mate):
        pl.semaphore_signal(barrier, inc=1, device_id={"sp": peer}, device_id_type=MESH)
    for k in range(1, n_tp):
        pl.semaphore_signal(barrier, inc=1, device_id={"tp": lax.rem(t + k, n_tp)}, device_id_type=MESH)

    lane = lax.broadcasted_iota(jnp.int32, (rows, LANES), 1)
    low = lane < 64
    grid_rows = rows // GRID_W
    first = me * grid_rows

    def table(j):
        pieces = []
        for g in range(grid_rows):
            r = row_tab[first + g][:, j * LANES : (j + 1) * LANES]
            pieces.append(col_tab[:, j * LANES : (j + 1) * LANES] + r)
        return jnp.concatenate(pieces, axis=0)

    def turn(x, j, shift):
        front = lax.rem(lane, 2 * shift) < shift
        other = jnp.where(front, pltpu.roll(x, LANES - shift, 1), pltpu.roll(x, shift, 1))
        return x * table(j) + other * table(j + 1)

    def norm_small(x, gain):
        sq = x * x
        lo = jnp.sum(jnp.where(low, sq, 0.0), axis=1, keepdims=True)
        hi = jnp.sum(jnp.where(low, 0.0, sq), axis=1, keepdims=True)
        scale = jnp.where(low, lax.rsqrt(lo / 64 + norm_eps), lax.rsqrt(hi / 64 + norm_eps))
        return x * scale * gain

    def norm_large(x, gain):
        return x * lax.rsqrt(jnp.mean(x * x, axis=1, keepdims=True) + norm_eps) * gain

    pair = jnp.concatenate([k_s[...], v_s[...]], axis=1).astype(F32)
    turned = turn(norm_small(pair, g_ks[...]), 0, 16)
    kv[me, :, 0:LANES] = jnp.where(low, turned, pair).astype(BF16)
    kv[me, :, LANES : 2 * LANES] = turn(norm_large(k_l[...].astype(F32), g_kl[...]), 2, 32).astype(BF16)
    kv[me, :, 2 * LANES : 3 * LANES] = v_l[...]
    pl.semaphore_wait(barrier, 2 + n_tp)

    def ring(direction, s, h):
        sign = 1 - 2 * direction
        block = at(z - sign * (s - 1))
        span = kv.at[block, pl.ds(h * half, half)]
        return pltpu.make_async_remote_copy(
            src_ref=span, dst_ref=span, send_sem=rs.at[direction, s, h], recv_sem=rr.at[direction, s, h],
            device_id={"sp": right if direction == 0 else left}, device_id_type=MESH,
        )

    def across(direction, s):
        sign = 1 - 2 * direction
        block = at(z - sign * s)
        return pltpu.make_async_remote_copy(
            src_ref=kv.at[block], dst_ref=kv.at[block], send_sem=ds.at[direction, s], recv_sem=dr.at[direction, s],
            device_id={"sp": mate}, device_id_type=MESH,
        )

    for h in range(2):
        ring(0, 1, h).start()
        ring(1, 1, h).start()
    across(0, 0).start()

    for p in range(n_small // 2):
        x = q_s[:, p * LANES : (p + 1) * LANES].astype(F32)
        y = turn(norm_small(x, g_qs[...]), 0, 16)
        q_all[2 * p] = jnp.where(low, y, 0.0).astype(BF16)
        q_all[2 * p + 1] = jnp.where(low, pltpu.roll(y, 64, 1), 0.0).astype(BF16)
    for p in range(n_large):
        x = q_l[:, p * LANES : (p + 1) * LANES].astype(F32)
        q_all[n_small + p] = turn(norm_large(x, g_ql[...]), 2, 32).astype(BF16)
    m_ref[...] = jnp.full_like(m_ref, far_below)
    l_ref[...] = jnp.zeros_like(l_ref)
    acc[...] = jnp.zeros_like(acc)

    def absorb(blocks):
        def group(g, k_at, v_at, factor):
            query = q_all[g]
            scores = [
                lax.dot_general(query, kv[b, :, k_at : k_at + LANES], (((1,), (1,)), ((), ())), preferred_element_type=F32)
                for b in blocks
            ]
            top = scores[0]
            for one in scores[1:]:
                top = jnp.maximum(top, one)
            old = m_ref[g][:, 0:1]
            new = jnp.maximum(old, jnp.max(top, axis=1, keepdims=True))
            shrink = jnp.exp2((old - new) * factor)
            total = None
            update = None
            for b, one in zip(blocks, scores):
                e = jnp.exp2((one - new) * factor)
                total = e if total is None else total + e
                piece = jnp.dot(e.astype(BF16), kv[b, :, v_at : v_at + LANES], preferred_element_type=F32)
                update = piece if update is None else update + piece
            m_ref[g] = jnp.broadcast_to(new, (rows, LANES))
            l_ref[g] = l_ref[g] * shrink + jnp.sum(total, axis=1, keepdims=True)
            acc[g] = acc[g] * shrink + update

        @pl.loop(0, n_small)
        def _(g):
            group(g, 0, 0, 64**-0.5 * LOG2E)

        @pl.loop(n_small, n_small + n_large)
        def _(g):
            group(g, LANES, 2 * LANES, 128**-0.5 * LOG2E)

    def pass_on(s, h):
        ring(0, s, h).wait_recv()
        ring(0, s + 1, h).start()
        ring(1, s, h).wait_recv()
        ring(1, s + 1, h).start()

    def step(s, blocks):
        for h in range(2):
            @pl.when(s < far - 1)
            def _():
                pass_on(s, h)

        @pl.when(s == far - 1)
        def _():
            ring(0, s, 0).wait_recv()
            ring(0, far, 0).start()
            ring(1, s, 0).wait_recv()
            ring(0, s, 1).wait_recv()
            ring(1, s, 1).wait_recv()
            ring(1, far, 1).start()

        @pl.when(s == far)
        def _():
            ring(0, far, 0).wait_recv()
            ring(1, far, 1).wait_recv()

        across(0, s).start()

        @pl.when(s < far)
        def _():
            across(1, s).start()

        across(0, s - 1).wait_recv()

        @pl.when(s > 1)
        def _():
            across(1, s - 1).wait_recv()

        absorb(blocks)

    def other(b):
        return b + 1 - 2 * c

    step(1, [me, other(me)])

    @pl.loop(2, far + 1)
    def _(s):
        a, b = at(z - s + 1), at(z + s - 1)
        step(s, [a, b, other(a), other(b)])

    across(0, far).wait_recv()
    last = at(z - far)
    absorb([last, other(last)])

    def finished(g):
        return acc[g] / l_ref[g]

    for p in range(n_small // 2):
        both = jnp.where(low, pltpu.roll(finished(2 * p), 64, 1), finished(2 * p + 1))
        heads[:, p * LANES : (p + 1) * LANES] = both.astype(BF16)
    for p in range(n_large):
        heads[:, (n_small // 2 + p) * LANES : (n_small // 2 + p + 1) * LANES] = finished(n_small + p).astype(BF16)

    width = resid.shape[1]
    n_cut = 4
    cut = width // n_cut
    split = n_small * 64

    def share(k, n):
        return pltpu.make_async_remote_copy(
            src_ref=part.at[n, lax.rem(t + k, n_tp)], dst_ref=got.at[n, k], send_sem=xs.at[n, k], recv_sem=xr.at[n, k],
            device_id={"tp": lax.rem(t + k, n_tp)}, device_id_type=MESH,
        )

    for n in range(n_cut):
        cols = slice(n * cut, (n + 1) * cut)
        whole = jnp.dot(heads[:, :split], w_s[:, cols], preferred_element_type=F32)
        whole = whole + jnp.dot(heads[:, split:], w_l[:, cols], preferred_element_type=F32)
        for d in range(n_tp):
            part[n, d] = whole[d * tok : (d + 1) * tok].astype(BF16)
        if n > 0:
            for k in (2, 1, 3):
                share(k, n - 1).start()
    for k in (2, 1, 3):
        share(k, n_cut - 1).start()
    squares = jnp.zeros((tok, 1), F32)
    for n in range(n_cut):
        cols = slice(n * cut, (n + 1) * cut)
        total = part[n, t].astype(F32)
        for k in range(1, n_tp):
            share(k, n).wait_recv()
            total = total + got[n, k].astype(F32)
        stream = (resid[:, cols].astype(F32) + total).astype(BF16)
        stream_out[:, cols] = stream
        wide = stream.astype(F32)
        squares = squares + jnp.sum(wide * wide, axis=1, keepdims=True)
    scale = lax.rsqrt(squares / width + norm_eps)
    normed_out[...] = (stream_out[...].astype(F32) * scale * g_ffn[...]).astype(BF16)

    @pl.loop(1, far)
    def _(s):
        for h in range(2):
            ring(0, s, h).wait_send()
            ring(1, s, h).wait_send()
        across(0, s).wait_send()
        across(1, s).wait_send()

    ring(0, far, 0).wait_send()
    ring(1, far, 1).wait_send()
    across(0, 0).wait_send()
    across(0, far).wait_send()
    for n in range(n_cut):
        for k in range(1, n_tp):
            share(k, n).wait_send()


def attention(q_s, k_s, v_s, q_l, k_l, v_l, gain_qs, gain_ks, gain_ql, gain_kl, w_s, w_l, resid, g_ffn):
    n_sp, n_tp = lax.axis_size("sp"), lax.axis_size("tp")
    chips = n_sp // 2
    rows = q_s.shape[0]
    rows_total = n_sp * rows // GRID_W
    tok, width = resid.shape
    groups = q_s.shape[1] // 64 + q_l.shape[1] // LANES
    (rc_s, rs_s), (cc_s, cs_s) = angle_tables(64, rows_total)
    (rc_l, rs_l), (cc_l, cs_l) = angle_tables(128, rows_total)
    row_tab = jnp.asarray(np.concatenate([rc_s, rs_s, rc_l, rs_l], axis=1)[:, None, :])
    col_tab = jnp.asarray(np.concatenate([cc_s, cs_s, cc_l, cs_l], axis=1))

    def twice(g):
        return jnp.concatenate([g, g]).reshape(1, LANES)

    far = chips // 2
    n_cut = 4
    dma = pltpu.SemaphoreType.DMA
    vmem = pl.BlockSpec(memory_space=pltpu.VMEM)
    return pl.pallas_call(
        functools.partial(attention_kernel, chips, n_tp),
        out_shape=[jax.ShapeDtypeStruct((tok, width), BF16)] * 2,
        in_specs=[vmem] * 16,
        out_specs=[vmem] * 2,
        scratch_shapes=[
            pltpu.VMEM((groups, rows, LANES), BF16),
            pltpu.VMEM((n_sp, rows, 3 * LANES), BF16),
            pltpu.VMEM((groups, rows, LANES), F32),
            pltpu.VMEM((groups, rows, LANES), F32),
            pltpu.VMEM((groups, rows, LANES), F32),
            pltpu.VMEM((rows, q_s.shape[1] + q_l.shape[1]), BF16),
            pltpu.VMEM((n_cut, n_tp, tok, width // n_cut), BF16),
            pltpu.VMEM((n_cut, n_tp, tok, width // n_cut), BF16),
            dma((2, far + 1, 2)), dma((2, far + 1, 2)),
            dma((2, far + 1)), dma((2, far + 1)),
            dma((n_cut, n_tp)), dma((n_cut, n_tp)),
        ],
        compiler_params=pltpu.CompilerParams(collective_id=0, has_side_effects=True, vmem_limit_bytes=48 * 2**20),
        name="attention",
    )(
        q_s, k_s, v_s, q_l, k_l, v_l, twice(gain_qs), twice(gain_ks), gain_ql.reshape(1, LANES), gain_kl.reshape(1, LANES),
        row_tab, col_tab, w_s, w_l, resid, g_ffn.reshape(1, -1),
    )


def cut_along(value, dim, length):
    dims = value.shape
    tiles = value.reshape(*dims[:dim], length, dims[dim] // length, *dims[dim + 1 :])
    return jnp.moveaxis(tiles, dim, 0)


def sum_at_owner(value, axis, dim):
    tiles = cut_along(value, dim, lax.axis_size(axis))
    arrived = lax.all_to_all(tiles, axis, split_axis=0, concat_axis=0, tiled=True)
    return arrived.astype(jnp.float32).sum(axis=0)


def local(
    residual_in,
    q_small,
    k_small,
    v_small,
    q_large,
    k_large,
    v_large,
    gain_qs,
    gain_ks,
    gain_ql,
    gain_kl,
    w_out_small,
    w_out_large,
    g_ffn,
    routes,
    route_w,
    w_gate,
    w_up,
    w_down,
    ws_gate,
    ws_up,
    ws_down,
):
    tp_count = lax.axis_size("tp")
    sp_count = lax.axis_size("sp")
    rows_dev = residual_in.shape[0]
    stream, normed = attention(
        q_small, k_small, v_small, q_large, k_large, v_large, gain_qs, gain_ks, gain_ql, gain_kl,
        w_out_small, w_out_large, residual_in, g_ffn,
    )
    stream32 = stream.astype(jnp.float32)
    channels = normed.shape[1]
    segment = lax.all_gather(normed, "tp", axis=0, tiled=True)
    gate_act = jnp.dot(segment, ws_gate, preferred_element_type=jnp.float32)
    up_act = jnp.dot(segment, ws_up, preferred_element_type=jnp.float32)
    hidden_shared = (jax.nn.silu(gate_act) * up_act).astype(jnp.bfloat16)
    shared = lax.psum_scatter(
        jnp.dot(hidden_shared, ws_down, preferred_element_type=jnp.float32).astype(jnp.bfloat16),
        "tp",
        scatter_dimension=0,
        tiled=True,
    ).astype(jnp.float32)
    local_experts = w_gate.shape[0]
    experts = local_experts * sp_count
    capacity = max(2, 2 * rows_dev * TOPK // experts)
    flat_ids = routes.reshape(-1)
    one_hot = (flat_ids[:, None] == jnp.arange(experts, dtype=jnp.int32)[None, :]).astype(jnp.int32)
    slot_ids = jnp.sum((jnp.cumsum(one_hot, axis=0) - 1) * one_hot, axis=1)
    targets = flat_ids * capacity + slot_ids
    owners = jnp.arange(rows_dev * TOPK, dtype=jnp.int32) // TOPK
    outbox = jnp.zeros((experts * capacity, channels), jnp.bfloat16).at[targets].set(normed[owners])
    arrived = lax.all_to_all(outbox, "sp", split_axis=0, concat_axis=0, tiled=True)
    arrived = lax.all_gather(
        arrived.reshape(sp_count, 1, local_experts, capacity, channels), "tp", axis=1, tiled=True
    )
    gate_act = jnp.einsum("abecd,edf->abecf", arrived, w_gate, preferred_element_type=jnp.float32)
    up_act = jnp.einsum("abecd,edf->abecf", arrived, w_up, preferred_element_type=jnp.float32)
    hidden = (jax.nn.silu(gate_act) * up_act).astype(jnp.bfloat16)
    partial_value = jnp.einsum(
        "abecf,efd->abecd", hidden, w_down, preferred_element_type=jnp.float32
    )
    summed = sum_at_owner(partial_value.astype(jnp.bfloat16), "tp", 1).astype(jnp.bfloat16)
    returned = lax.all_to_all(
        summed.reshape(sp_count * local_experts * capacity, channels),
        "sp",
        split_axis=0,
        concat_axis=0,
        tiled=True,
    )
    picked = returned[targets].reshape(rows_dev, TOPK, channels).astype(jnp.float32)
    routed = jnp.sum(picked * route_w[..., None], axis=1)
    return (stream32 + routed + shared).astype(jnp.bfloat16)


def solution(mesh):
    placed = (
        P(("grp", "sp", "tp"), None),
        P(("grp", "sp"), "tp"),
        P(("grp", "sp"), "tp"),
        P(("grp", "sp"), "tp"),
        P(("grp", "sp"), "tp"),
        P(("grp", "sp"), "tp"),
        P(("grp", "sp"), "tp"),
        P(),
        P(),
        P(),
        P(),
        P("tp", None),
        P("tp", None),
        P(),
        P(("grp", "sp", "tp"), None),
        P(("grp", "sp", "tp"), None),
        P("sp", None, "tp"),
        P("sp", None, "tp"),
        P("sp", "tp", None),
        P(None, "tp"),
        P(None, "tp"),
        P("tp", None),
    )
    return jax.shard_map(
        local, mesh=mesh, in_specs=placed, out_specs=P(("grp", "sp", "tp"), None), check_vma=False
    )
```

```python
import functools
import math

import jax
import jax.numpy as jnp
import numpy as np
from jax import lax
from jax.experimental import pallas as pl
from jax.experimental.pallas import tpu as pltpu
from jax.sharding import PartitionSpec as P

GRID_W = 64
TOPK = 4
norm_eps = 1e-06
rope_base = 10000.0
far_below = -1e30
LANES = 128
LOG2E = math.log2(math.e)
MESH = pl.DeviceIdType.MESH
F32 = jnp.float32
BF16 = jnp.bfloat16


def angle_tables(channels, rows_total):
    quarter = channels // 4
    lane = np.arange(LANES) % channels
    by_row = lane < channels // 2
    front = lane % (channels // 2) < quarter
    inverse = (1.0 / rope_base ** (np.arange(quarter, dtype=np.float32) / np.float32(quarter))).astype(np.float32)
    freq = inverse[lane % quarter]

    def tables(count, mask):
        angle = np.arange(count, dtype=np.float32)[:, None] * freq[None, :]
        angle = angle.astype(np.float32).astype(np.float64)
        cosine = np.where(mask[None, :], np.cos(angle), 0.0)
        sine = np.where(mask[None, :], np.where(front[None, :], -np.sin(angle), np.sin(angle)), 0.0)
        return cosine.astype(np.float32), sine.astype(np.float32)

    return tables(rows_total, by_row), tables(GRID_W, ~by_row)


def layer_kernel(
    chips, n_tp,
    q_s_in, kt_in, vt_in, q_l_in, k_l_in, v_l_in, g_qs_in, g_ks_in, g_ql_in, g_kl_in, g_ffn_in, row_in, col_in,
    w_s_in, w_l_in, resid_in, routes_in, route_w_in, w_gate, w_up, w_down, ws_gate_in, ws_up_in, ws_down_in,
    result,
    q_s, kt, vt, q_l, k_l, v_l, g_qs, g_ks, g_ql, g_kl, g_ffn, row_tab, col_tab, w_s, w_l, resid, routes, route_w,
    ws_gate, ws_up, ws_down,
    q_all, kv, m_ref, l_ref, acc, heads, part, got,
    stream_ref, meta, tok, wg, wu, wd, sel, rows_in, outs, res, rs_in, stok, spart, sgot, big, own, cbuf,
    load, rs, rr, ds, dr, xs, xr,
    ms, mr, ts, tr, gs, gr, es, er, bs, br, ss, sr, ps, pr, wsnd, wrcv, fs, fr, wl,
):
    me = lax.axis_index("sp")
    t = lax.axis_index("tp")
    z = me // 2
    c = me % 2
    rows = q_s.shape[0]
    half = rows // 2
    far = chips // 2
    n_tok = resid.shape[0]
    n_small = q_s.shape[1] // 64
    n_large = q_l.shape[1] // LANES

    def at(zz):
        return lax.rem(zz + 2 * chips, chips) * 2 + c

    right, left, mate = at(z + 1), at(z - 1), z * 2 + (1 - c)

    pairs = [
        (kt_in, kt), (vt_in, vt), (k_l_in, k_l), (v_l_in, v_l), (g_ks_in, g_ks), (g_kl_in, g_kl), (row_in, row_tab),
        (col_in, col_tab), (q_s_in, q_s), (q_l_in, q_l), (g_qs_in, g_qs), (g_ql_in, g_ql), (routes_in, routes),
        (route_w_in, route_w), (g_ffn_in, g_ffn), (resid_in, resid), (w_s_in, w_s), (w_l_in, w_l),
        (ws_gate_in, ws_gate), (ws_up_in, ws_up), (ws_down_in, ws_down),
    ]
    loads = [pltpu.make_async_copy(src, dst, load.at[i]) for i, (src, dst) in enumerate(pairs)]
    for one in loads:
        one.start()
    barrier = pltpu.get_barrier_semaphore()
    for peer in (right, left, mate):
        pl.semaphore_signal(barrier, inc=1, device_id={"sp": peer}, device_id_type=MESH)
    for k in range(1, n_tp):
        pl.semaphore_signal(barrier, inc=1, device_id={"tp": lax.rem(t + k, n_tp)}, device_id_type=MESH)

    for one in loads[:8]:
        one.wait()
    lane = lax.broadcasted_iota(jnp.int32, (rows, LANES), 1)
    low = lane < 64
    grid_rows = rows // GRID_W
    first = me * grid_rows

    def table(j):
        pieces = []
        for g in range(grid_rows):
            r = row_tab[first + g][:, j * LANES : (j + 1) * LANES]
            pieces.append(col_tab[:, j * LANES : (j + 1) * LANES] + r)
        return jnp.concatenate(pieces, axis=0)

    def turn(x, j, shift):
        front = lax.rem(lane, 2 * shift) < shift
        other = jnp.where(front, pltpu.roll(x, LANES - shift, 1), pltpu.roll(x, shift, 1))
        return x * table(j) + other * table(j + 1)

    def norm_small(x, gain):
        sq = x * x
        lo = jnp.sum(jnp.where(low, sq, 0.0), axis=1, keepdims=True)
        hi = jnp.sum(jnp.where(low, 0.0, sq), axis=1, keepdims=True)
        scale = jnp.where(low, lax.rsqrt(lo / 64 + norm_eps), lax.rsqrt(hi / 64 + norm_eps))
        return x * scale * gain

    def norm_large(x, gain):
        return x * lax.rsqrt(jnp.mean(x * x, axis=1, keepdims=True) + norm_eps) * gain

    def twice(g):
        return jnp.concatenate([g[...], g[...]], axis=1)

    pair = jnp.concatenate([kt[...].astype(F32).T, vt[...].astype(F32).T], axis=1)
    turned = turn(norm_small(pair, twice(g_ks)), 0, 16)
    kv[me, :, 0:LANES] = jnp.where(low, turned, pair).astype(BF16)
    kv[me, :, LANES : 2 * LANES] = turn(norm_large(k_l[...].astype(F32), g_kl[...]), 2, 32).astype(BF16)
    kv[me, :, 2 * LANES : 3 * LANES] = v_l[...]
    pl.semaphore_wait(barrier, 2 + n_tp)

    def ring(direction, s, h):
        sign = 1 - 2 * direction
        block = at(z - sign * (s - 1))
        span = kv.at[block, pl.ds(h * half, half)]
        return pltpu.make_async_remote_copy(
            src_ref=span, dst_ref=span, send_sem=rs.at[direction, s, h], recv_sem=rr.at[direction, s, h],
            device_id={"sp": right if direction == 0 else left}, device_id_type=MESH,
        )

    def across(direction, s):
        sign = 1 - 2 * direction
        block = at(z - sign * s)
        return pltpu.make_async_remote_copy(
            src_ref=kv.at[block], dst_ref=kv.at[block], send_sem=ds.at[direction, s], recv_sem=dr.at[direction, s],
            device_id={"sp": mate}, device_id_type=MESH,
        )

    for h in range(2):
        ring(0, 1, h).start()
        ring(1, 1, h).start()
    across(0, 0).start()

    holder = c == t // 2
    n_q = 8
    moved = [(w_gate, wg, w_gate.shape[1] // n_q), (w_up, wu, w_up.shape[1] // n_q), (w_down, wd, w_down.shape[1] // n_q)]

    def weight_copy(m, q, k):
        src, dst, span = moved[m]
        aim = lax.rem(t + k, n_tp)
        piece = pl.ds(q * span, span)
        return pltpu.make_async_remote_copy(
            src_ref=src.at[lax.rem(aim, 2), piece], dst_ref=dst.at[t, piece], send_sem=wsnd.at[m, q, k],
            recv_sem=wrcv.at[m, q, k], device_id={"tp": aim}, device_id_type=MESH,
        )

    def weight_in(m, q, k):
        src, dst, span = moved[m]
        piece = pl.ds(q * span, span)
        home = dst.at[lax.rem(t + n_tp - k, n_tp), piece]
        return pltpu.make_async_remote_copy(
            src_ref=home, dst_ref=home, send_sem=wsnd.at[m, q, k],
            recv_sem=wrcv.at[m, q, k], device_id={"tp": lax.rem(t + k, n_tp)}, device_id_type=MESH,
        )

    def weight_on(m, q, k):
        src, dst, span = moved[m]
        piece = pl.ds(q * span, span)
        home = dst.at[lax.rem(t + n_tp - k, n_tp), piece]
        return pltpu.make_async_remote_copy(
            src_ref=home, dst_ref=home, send_sem=fs.at[m, q, k], recv_sem=fr.at[m, q, k],
            device_id={"sp": mate}, device_id_type=MESH,
        )

    def weight_mine(m):
        src, dst, _ = moved[m]
        return pltpu.make_async_copy(src.at[lax.rem(t, 2)], dst.at[t], wl.at[m])

    def weight_to_mate(m):
        src, dst, _ = moved[m]
        return pltpu.make_async_remote_copy(
            src_ref=src.at[lax.rem(t, 2)], dst_ref=dst.at[t], send_sem=fs.at[m, 0, 0], recv_sem=fr.at[m, 0, 0],
            device_id={"sp": mate}, device_id_type=MESH,
        )

    def carry_weights(q):
        for k in range(1, n_tp):
            @pl.when(c == lax.rem(t + k, n_tp) // 2)
            def _():
                for m in range(3):
                    weight_copy(m, q, k).start()

    def relay_weights(q):
        @pl.when(holder)
        def _():
            for m in range(3):
                for k in range(1, n_tp):
                    weight_in(m, q, k).wait_recv()
                    weight_on(m, q, k).start()

    @pl.when(holder)
    def _():
        for m in range(3):
            weight_mine(m).start()
            weight_to_mate(m).start()

    carry_weights(0)
    for one in loads[8:14]:
        one.wait()

    slots = result.shape[0] // 8
    experts = n_tp * chips
    ex = lax.broadcasted_iota(jnp.int32, (experts, n_tok), 0)
    hits = [ex == routes[j : j + 1, :] for j in range(TOPK)]
    named = hits[0]
    for one in hits[1:]:
        named = named | one
    before = lax.broadcasted_iota(jnp.int32, (n_tok, n_tok), 0) < lax.broadcasted_iota(jnp.int32, (n_tok, n_tok), 1)
    ahead = jnp.dot(
        jnp.where(named, 1.0, 0.0).astype(BF16), jnp.where(before, 1.0, 0.0).astype(BF16), preferred_element_type=F32
    )
    meta[z] = jnp.zeros(meta.shape[1:], F32)
    for j in range(TOPK):
        place = jnp.sum(jnp.where(hits[j], ahead, 0.0), axis=0, keepdims=True)
        code = routes[j : j + 1, :].astype(F32) * slots + place
        meta[z, j : j + 1, :] = jnp.concatenate([code, code], axis=1)
    meta[z, 8 : 8 + TOPK, :] = jnp.concatenate([route_w[...], route_w[...]], axis=1)

    for p in range(n_small // 2):
        x = q_s[:, p * LANES : (p + 1) * LANES].astype(F32)
        y = turn(norm_small(x, twice(g_qs)), 0, 16)
        q_all[2 * p] = jnp.where(low, y, 0.0).astype(BF16)
        q_all[2 * p + 1] = jnp.where(low, pltpu.roll(y, 64, 1), 0.0).astype(BF16)
    for p in range(n_large):
        x = q_l[:, p * LANES : (p + 1) * LANES].astype(F32)
        q_all[n_small + p] = turn(norm_large(x, g_ql[...]), 2, 32).astype(BF16)
    m_ref[...] = jnp.full_like(m_ref, far_below)
    l_ref[...] = jnp.zeros_like(l_ref)
    acc[...] = jnp.zeros_like(acc)

    def meta_ring(direction, s):
        sign = 1 - 2 * direction
        block = lax.rem(z - sign * (s - 1) + 2 * chips, chips)
        return pltpu.make_async_remote_copy(
            src_ref=meta.at[block], dst_ref=meta.at[block], send_sem=ms.at[direction, s], recv_sem=mr.at[direction, s],
            device_id={"sp": right if direction == 0 else left}, device_id_type=MESH,
        )

    meta_ring(0, 1).start()
    meta_ring(1, 1).start()

    def absorb(blocks):
        def group(g, k_at, v_at, factor):
            query = q_all[g]
            scores = [
                lax.dot_general(query, kv[b, :, k_at : k_at + LANES], (((1,), (1,)), ((), ())), preferred_element_type=F32)
                for b in blocks
            ]
            top = scores[0]
            for one in scores[1:]:
                top = jnp.maximum(top, one)
            old = m_ref[g][:, 0:1]
            new = jnp.maximum(old, jnp.max(top, axis=1, keepdims=True))
            shrink = jnp.exp2((old - new) * factor)
            total = None
            update = None
            for b, one in zip(blocks, scores):
                e = jnp.exp2((one - new) * factor)
                total = e if total is None else total + e
                piece = jnp.dot(e.astype(BF16), kv[b, :, v_at : v_at + LANES], preferred_element_type=F32)
                update = piece if update is None else update + piece
            m_ref[g] = jnp.broadcast_to(new, (rows, LANES))
            l_ref[g] = l_ref[g] * shrink + jnp.sum(total, axis=1, keepdims=True)
            acc[g] = acc[g] * shrink + update

        @pl.loop(0, n_small)
        def _(g):
            group(g, 0, 0, 64**-0.5 * LOG2E)

        @pl.loop(n_small, n_small + n_large)
        def _(g):
            group(g, LANES, 2 * LANES, 128**-0.5 * LOG2E)

    def pass_on(s, h):
        ring(0, s, h).wait_recv()
        ring(0, s + 1, h).start()
        ring(1, s, h).wait_recv()
        ring(1, s + 1, h).start()

    def step(s, blocks):
        for h in range(2):
            @pl.when(s < far - 1)
            def _():
                pass_on(s, h)

        @pl.when(s == far - 1)
        def _():
            ring(0, s, 0).wait_recv()
            ring(0, far, 0).start()
            ring(1, s, 0).wait_recv()
            ring(0, s, 1).wait_recv()
            ring(1, s, 1).wait_recv()
            ring(1, far, 1).start()

        @pl.when(s == far)
        def _():
            ring(0, far, 0).wait_recv()
            ring(1, far, 1).wait_recv()

        across(0, s).start()
        meta_ring(0, s).wait_recv()

        @pl.when(s < far)
        def _():
            across(1, s).start()
            meta_ring(1, s).wait_recv()
            meta_ring(0, s + 1).start()

        @pl.when(s < far - 1)
        def _():
            meta_ring(1, s + 1).start()

        for q in range(1, 4):
            @pl.when(s == 2 * q)
            def _():
                carry_weights(q)

        across(0, s - 1).wait_recv()

        @pl.when(s > 1)
        def _():
            across(1, s - 1).wait_recv()

        absorb(blocks)

    def other(b):
        return b + 1 - 2 * c

    step(1, [me, other(me)])

    @pl.loop(2, far + 1)
    def _(s):
        a, b = at(z - s + 1), at(z + s - 1)
        step(s, [a, b, other(a), other(b)])

    across(0, far).wait_recv()
    last = at(z - far)
    absorb([last, other(last)])

    for one in loads[14:18]:
        one.wait()

    def finished(g):
        return acc[g] / l_ref[g]

    for p in range(n_small // 2):
        both = jnp.where(low, pltpu.roll(finished(2 * p), 64, 1), finished(2 * p + 1))
        heads[:, p * LANES : (p + 1) * LANES] = both.astype(BF16)
    for p in range(n_large):
        heads[:, (n_small // 2 + p) * LANES : (n_small // 2 + p + 1) * LANES] = finished(n_small + p).astype(BF16)

    width = resid.shape[1]
    n_cut = 4
    cut = width // n_cut
    split = n_small * 64

    def share(k, n):
        return pltpu.make_async_remote_copy(
            src_ref=part.at[n, lax.rem(t + k, n_tp)], dst_ref=got.at[n, k], send_sem=xs.at[n, k], recv_sem=xr.at[n, k],
            device_id={"tp": lax.rem(t + k, n_tp)}, device_id_type=MESH,
        )

    for n in range(n_cut):
        cols = slice(n * cut, (n + 1) * cut)
        whole = jnp.dot(heads[:, :split], w_s[:, cols], preferred_element_type=F32)
        whole = whole + jnp.dot(heads[:, split:], w_l[:, cols], preferred_element_type=F32)
        for d in range(n_tp):
            part[n, d] = whole[d * n_tok : (d + 1) * n_tok].astype(BF16)
        if n > 0:
            for k in (2, 1, 3):
                share(k, n - 1).start()
    for k in (2, 1, 3):
        share(k, n_cut - 1).start()
    squares = jnp.zeros((n_tok, 1), F32)
    for n in range(n_cut):
        cols = slice(n * cut, (n + 1) * cut)
        total = part[n, t].astype(F32)
        for k in range(1, n_tp):
            share(k, n).wait_recv()
            total = total + got[n, k].astype(F32)
        stream = (resid[:, cols].astype(F32) + total).astype(BF16)
        stream_ref[:, cols] = stream
        wide = stream.astype(F32)
        squares = squares + jnp.sum(wide * wide, axis=1, keepdims=True)
    scale = lax.rsqrt(squares / width + norm_eps)
    tok[z] = (stream_ref[...].astype(F32) * scale * g_ffn[...]).astype(BF16)

    tok_half = n_tok // 2

    def zmod(v):
        return lax.rem(v + 2 * chips, chips)

    def token_ring(direction, s, h):
        sign = 1 - 2 * direction
        span = tok.at[zmod(z - sign * (s - 1)), pl.ds(h * tok_half, tok_half)]
        return pltpu.make_async_remote_copy(
            src_ref=span, dst_ref=span, send_sem=ts.at[direction, s, h], recv_sem=tr.at[direction, s, h],
            device_id={"sp": right if direction == 0 else left}, device_id_type=MESH,
        )

    for h in range(2):
        token_ring(0, 1, h).start()
        token_ring(1, 1, h).start()
    carry_weights(4)

    wide_lane = lax.broadcasted_iota(jnp.int32, (8 * slots, LANES), 1)
    wide_row = lax.broadcasted_iota(jnp.int32, (8 * slots, LANES), 0)
    second_token = wide_lane // n_tok
    second_row = lax.rem(wide_row // slots, 2)
    code_row = (z * n_tp + wide_row // (2 * slots)) * slots + lax.rem(wide_row, slots)
    code_row = jnp.where(second_token == second_row, code_row, -1).astype(F32)

    def blocks_of(g):
        last = g == far
        return jnp.where(last, z, zmod(z - g)), zmod(z + g)

    def codes(g):
        a, b = blocks_of(g)
        return jnp.where(lax.broadcasted_iota(jnp.int32, meta.shape[1:], 1) < n_tok, meta[a], meta[b])

    def dispatch(g, k):
        return pltpu.make_async_remote_copy(
            src_ref=sel.at[g - 1, lax.rem(t + k, n_tp)], dst_ref=rows_in.at[g - 1, t], send_sem=gs.at[g, k],
            recv_sem=gr.at[g, k], device_id={"tp": lax.rem(t + k, n_tp)}, device_id_type=MESH,
        )

    def give_back(g, k):
        return pltpu.make_async_remote_copy(
            src_ref=outs.at[g - 1, lax.rem(t + k, n_tp)], dst_ref=res.at[g - 1, t], send_sem=es.at[g, k],
            recv_sem=er.at[g, k], device_id={"tp": lax.rem(t + k, n_tp)}, device_id_type=MESH,
        )

    def pick(g):
        a, b = blocks_of(g)
        code = codes(g)
        chosen = jnp.zeros(wide_row.shape, F32)
        for j in range(TOPK):
            chosen = chosen + jnp.where(code[j : j + 1, :] == code_row, 1.0, 0.0)
        chosen = chosen.astype(BF16)
        both = jnp.concatenate([tok[a], tok[b]], axis=0)
        picked = jnp.dot(chosen, both, preferred_element_type=F32).astype(BF16)
        for i in range(n_tp):
            sel[g - 1, i] = picked[i * 2 * slots : (i + 1) * 2 * slots]
        rows_in[g - 1, t] = sel[g - 1, t]
        for k in (2, 1, 3):
            dispatch(g, k).start()

    def token_step(s):
        for h in range(2):
            @pl.when(s < far - 1)
            def _():
                for d in range(2):
                    token_ring(d, s, h).wait_recv()
                    token_ring(d, s + 1, h).start()

        @pl.when(s == far - 1)
        def _():
            token_ring(0, s, 0).wait_recv()
            token_ring(0, far, 0).start()
            token_ring(1, s, 0).wait_recv()
            token_ring(0, s, 1).wait_recv()
            token_ring(1, s, 1).wait_recv()
            token_ring(1, far, 1).start()

        @pl.when(s == far)
        def _():
            token_ring(0, far, 0).wait_recv()
            token_ring(1, far, 1).wait_recv()

    @pl.loop(1, far + 1)
    def _(s):
        token_step(s)
        for q in range(5, n_q):
            @pl.when(s == q - 4)
            def _():
                carry_weights(q)
        pick(s)
        relay_weights(s - 1)

    @pl.when(holder)
    def _():
        for m in range(3):
            weight_mine(m).wait()

    @pl.when(jnp.logical_not(holder))
    def _():
        for m in range(3):
            weight_to_mate(m).wait_recv()

            @pl.loop(0, n_q)
            def _(q):
                for k in range(1, n_tp):
                    weight_on(m, q, k).wait_recv()

    batch = far // 2
    for first_group in (batch + 1, 1):
        @pl.loop(first_group, first_group + batch)
        def _(g):
            for k in range(1, n_tp):
                dispatch(g, k).wait_recv()

        x = rows_in[first_group - 1 : first_group - 1 + batch].reshape(batch * n_tp * 2 * slots, width)
        big[...] = jnp.zeros_like(big)

        @pl.loop(0, n_tp)
        def _(j):
            gate = jnp.dot(x, wg[j], preferred_element_type=F32)
            up = jnp.dot(x, wu[j], preferred_element_type=F32)
            hidden = (gate / (1.0 + jnp.exp(-gate)) * up).astype(BF16)
            big[...] += jnp.dot(hidden, wd[j], preferred_element_type=F32)

        for n in range(batch - 1, -1, -1):
            g = first_group + n
            for i in range(n_tp):
                at_row = (n * n_tp + i) * 2 * slots
                outs[g - 1, i] = big[at_row : at_row + 2 * slots, :].astype(BF16)
            res[g - 1, t] = outs[g - 1, t]
            for k in (2, 1, 3):
                give_back(g, k).start()

    def share_tokens(k):
        return pltpu.make_async_remote_copy(
            src_ref=tok.at[z], dst_ref=stok.at[t], send_sem=ss.at[k], recv_sem=sr.at[k],
            device_id={"tp": lax.rem(t + k, n_tp)}, device_id_type=MESH,
        )

    def share_back(k):
        return pltpu.make_async_remote_copy(
            src_ref=spart.at[lax.rem(t + k, n_tp)], dst_ref=sgot.at[t], send_sem=ps.at[k], recv_sem=pr.at[k],
            device_id={"tp": lax.rem(t + k, n_tp)}, device_id_type=MESH,
        )

    for one in loads[18:]:
        one.wait()
    stok[t] = tok[z]
    for k in (2, 1, 3):
        share_tokens(k).start()

    @pl.loop(1, far)
    def _(s):
        for h in range(2):
            token_ring(0, s, h).wait_send()
            token_ring(1, s, h).wait_send()

    token_ring(0, far, 0).wait_send()
    token_ring(1, far, 1).wait_send()
    for k in range(1, n_tp):
        share_tokens(k).wait_send()

    def sum_ring(direction, i, h):
        piece = pl.ds(h * tok_half, tok_half)
        return pltpu.make_async_remote_copy(
            src_ref=tok.at[direction * far + i - 1, piece], dst_ref=rs_in.at[direction, i - 1, piece],
            send_sem=bs.at[direction, i, h], recv_sem=br.at[direction, i, h],
            device_id={"sp": right if direction == 0 else left}, device_id_type=MESH,
        )

    def weigh(g):
        for k in range(1, n_tp):
            give_back(g, k).wait_recv()
        code = codes(g)
        weight = jnp.zeros(wide_row.shape, F32)
        for j in range(TOPK):
            weight = weight + jnp.where(code[j : j + 1, :] == code_row, code[8 + j : 9 + j, :], 0.0)
        high = weight.astype(BF16)
        rest = weight - high.astype(F32)
        across_rows = jnp.concatenate([high.astype(F32), rest], axis=0).T.astype(BF16)
        back = res[g - 1].reshape(n_tp * 2 * slots, width)
        cbuf[...] = jnp.dot(across_rows, jnp.concatenate([back, back], axis=0), preferred_element_type=F32)

    weigh(far)
    own[...] = cbuf[0:n_tok, :]
    tok[0, 0:tok_half] = cbuf[n_tok : n_tok + tok_half, :].astype(BF16)
    tok[far, tok_half : 2 * tok_half] = cbuf[n_tok + tok_half : 2 * n_tok, :].astype(BF16)
    sum_ring(0, 1, 0).start()
    sum_ring(1, 1, 1).start()

    def send_sum(direction, i, h, add):
        begin = (1 - direction) * n_tok + h * tok_half
        value = cbuf[begin : begin + tok_half, :]
        if add:
            sum_ring(direction, i - 1, h).wait_recv()
            value = value + rs_in[direction, i - 2, h * tok_half : (h + 1) * tok_half].astype(F32)
        tok[direction * far + i - 1, h * tok_half : (h + 1) * tok_half] = value.astype(BF16)
        sum_ring(direction, i, h).start()

    weigh(far - 1)
    send_sum(0, 2, 1, False)
    send_sum(1, 2, 0, False)
    send_sum(0, 2, 0, True)
    send_sum(1, 2, 1, True)

    @pl.loop(3, far + 1)
    def _(i):
        weigh(far + 1 - i)
        for h in range(2):
            for direction in range(2):
                send_sum(direction, i, 1 - h if direction == 0 else h, True)

        @pl.when(i == 4)
        def _():
            for k in range(1, n_tp):
                share_tokens(k).wait_recv()
            x = stok[...].reshape(n_tp * n_tok, width)
            gate = jnp.dot(x, ws_gate[...], preferred_element_type=F32)
            up = jnp.dot(x, ws_up[...], preferred_element_type=F32)
            hidden = (gate / (1.0 + jnp.exp(-gate)) * up).astype(BF16)
            big[...] = jnp.dot(hidden, ws_down[...], preferred_element_type=F32)
            for d in range(n_tp):
                spart[d] = big[d * n_tok : (d + 1) * n_tok, :].astype(BF16)
            sgot[t] = spart[t]
            for k in (2, 1, 3):
                share_back(k).start()

    for k in range(1, n_tp):
        share_back(k).wait_recv()
    total = stream_ref[...].astype(F32) + own[...]
    for d in range(n_tp):
        total = total + sgot[d].astype(F32)
    own[...] = total
    for h in range(2):
        piece = slice(h * tok_half, (h + 1) * tok_half)
        for direction in range(2):
            sum_ring(direction, far, h).wait_recv()
        result[piece, :] = (
            own[piece, :] + rs_in[0, far - 1, piece].astype(F32) + rs_in[1, far - 1, piece].astype(F32)
        ).astype(BF16)

    @pl.loop(1, far)
    def _(s):
        for h in range(2):
            ring(0, s, h).wait_send()
            ring(1, s, h).wait_send()
        across(0, s).wait_send()
        across(1, s).wait_send()

    ring(0, far, 0).wait_send()
    ring(1, far, 1).wait_send()
    across(0, 0).wait_send()
    across(0, far).wait_send()
    for n in range(n_cut):
        for k in range(1, n_tp):
            share(k, n).wait_send()

    @pl.loop(2, far + 1)
    def _(i):
        for h in range(2):
            for d in range(2):
                sum_ring(d, i, h).wait_send()

    sum_ring(0, 1, 0).wait_send()
    sum_ring(1, 1, 1).wait_send()
    for k in range(1, n_tp):
        share_back(k).wait_send()

        @pl.loop(1, far + 1)
        def _(g):
            dispatch(g, k).wait_send()
            give_back(g, k).wait_send()

        @pl.when(c == lax.rem(t + k, n_tp) // 2)
        def _():
            @pl.loop(0, n_q)
            def _(q):
                for m in range(3):
                    weight_copy(m, q, k).wait_send()

    @pl.when(holder)
    def _():
        for m in range(3):
            weight_to_mate(m).wait_send()

            @pl.loop(0, n_q)
            def _(q):
                for k in range(1, n_tp):
                    weight_on(m, q, k).wait_send()

    @pl.loop(1, far + 1)
    def _(s):
        meta_ring(0, s).wait_send()

    @pl.loop(1, far)
    def _(s):
        meta_ring(1, s).wait_send()


def layer(
    residual_in, q_small, k_small, v_small, q_large, k_large, v_large, gain_qs, gain_ks, gain_ql, gain_kl,
    w_out_small, w_out_large, g_ffn, routes, route_w, w_gate, w_up, w_down, ws_gate, ws_up, ws_down,
):
    n_sp, n_tp = lax.axis_size("sp"), lax.axis_size("tp")
    chips = n_sp // 2
    far = chips // 2
    rows = q_small.shape[0]
    rows_total = n_sp * rows // GRID_W
    tok, width = residual_in.shape
    groups = q_small.shape[1] // 64 + q_large.shape[1] // LANES
    slots = max(2, 2 * tok * TOPK // (w_gate.shape[0] * n_sp))
    assert w_gate.shape[0] * 2 == n_tp and 2 * tok == LANES and slots == 8
    (rc_s, rs_s), (cc_s, cs_s) = angle_tables(64, rows_total)
    (rc_l, rs_l), (cc_l, cs_l) = angle_tables(128, rows_total)
    row_tab = jnp.asarray(np.concatenate([rc_s, rs_s, rc_l, rs_l], axis=1)[:, None, :])
    col_tab = jnp.asarray(np.concatenate([cc_s, cs_s, cc_l, cs_l], axis=1))
    operands = [
        q_small, k_small.T, v_small.T, q_large, k_large, v_large, gain_qs.reshape(1, -1), gain_ks.reshape(1, -1),
        gain_ql.reshape(1, -1), gain_kl.reshape(1, -1), g_ffn.reshape(1, -1), row_tab, col_tab, w_out_small, w_out_large,
        residual_in, routes.T, route_w.T, w_gate, w_up, w_down, ws_gate, ws_up, ws_down,
    ]
    n_cut, n_q, batch = 4, 8, far // 2
    dma = pltpu.SemaphoreType.DMA
    copies = [pltpu.VMEM(x.shape, x.dtype) for x in operands[:18] + operands[21:]]

    def bf(*shape):
        return pltpu.VMEM(shape, BF16)

    def f32(*shape):
        return pltpu.VMEM(shape, F32)

    moved_rows = (far, n_tp, 2 * slots, width)
    return pl.pallas_call(
        functools.partial(layer_kernel, chips, n_tp),
        out_shape=jax.ShapeDtypeStruct((tok, width), BF16),
        in_specs=[pl.BlockSpec(memory_space=pl.ANY)] * len(operands),
        out_specs=pl.BlockSpec(memory_space=pltpu.VMEM),
        scratch_shapes=copies + [
            bf(groups, rows, LANES), bf(n_sp, rows, 3 * LANES), f32(groups, rows, LANES), f32(groups, rows, LANES),
            f32(groups, rows, LANES), bf(rows, q_small.shape[1] + q_large.shape[1]),
            bf(n_cut, n_tp, tok, width // n_cut), bf(n_cut, n_tp, tok, width // n_cut),
            bf(tok, width), f32(chips, 16, LANES), bf(chips, tok, width),
            bf(n_tp, *w_gate.shape[1:]), bf(n_tp, *w_up.shape[1:]), bf(n_tp, *w_down.shape[1:]),
            bf(*moved_rows), bf(*moved_rows), bf(*moved_rows), bf(*moved_rows), bf(2, far, tok, width),
            bf(n_tp, tok, width), bf(n_tp, tok, width), bf(n_tp, tok, width),
            f32(batch * n_tp * 2 * slots, width), f32(tok, width), f32(2 * tok, width),
            dma((len(copies),)),
            dma((2, far + 1, 2)), dma((2, far + 1, 2)), dma((2, far + 1)), dma((2, far + 1)), dma((n_cut, n_tp)), dma((n_cut, n_tp)),
            dma((2, far + 1)), dma((2, far + 1)), dma((2, far + 1, 2)), dma((2, far + 1, 2)),
            dma((far + 1, n_tp)), dma((far + 1, n_tp)), dma((far + 1, n_tp)), dma((far + 1, n_tp)),
            dma((2, far + 1, 2)), dma((2, far + 1, 2)), dma((n_tp,)), dma((n_tp,)), dma((n_tp,)), dma((n_tp,)),
            dma((3, n_q, n_tp)), dma((3, n_q, n_tp)), dma((3, n_q, n_tp)), dma((3, n_q, n_tp)), dma((3,)),
        ],
        compiler_params=pltpu.CompilerParams(collective_id=0, has_side_effects=True, vmem_limit_bytes=67_043_328),
        name="layer",
    )(*operands)


def solution(mesh):
    part = P(("grp", "sp"), "tp")
    each = P(("grp", "sp", "tp"), None)
    placed = (
        each, part, part, part, part, part, part, P(), P(), P(), P(), P("tp", None), P("tp", None), P(), each, each,
        P("sp", None, "tp"), P("sp", None, "tp"), P("sp", "tp", None), P(None, "tp"), P(None, "tp"), P("tp", None),
    )
    return jax.shard_map(layer, mesh=mesh, in_specs=placed, out_specs=each, check_vma=False)
```

```python
import functools
import math

import jax
import jax.numpy as jnp
import numpy as np
from jax import lax
from jax.experimental import pallas as pl
from jax.experimental.pallas import tpu as pltpu
from jax.sharding import PartitionSpec as P

GRID_W = 64
TOPK = 4
norm_eps = 1e-06
rope_base = 10000.0
far_below = -1e30
LANES = 128
LOG2E = math.log2(math.e)
MESH = pl.DeviceIdType.MESH
F32 = jnp.float32
BF16 = jnp.bfloat16


def angle_tables(channels, rows_total):
    quarter = channels // 4
    lane = np.arange(LANES) % channels
    by_row = lane < channels // 2
    front = lane % (channels // 2) < quarter
    inverse = (1.0 / rope_base ** (np.arange(quarter, dtype=np.float32) / np.float32(quarter))).astype(np.float32)
    freq = inverse[lane % quarter]

    def tables(count, mask):
        angle = np.arange(count, dtype=np.float32)[:, None] * freq[None, :]
        angle = angle.astype(np.float32).astype(np.float64)
        cosine = np.where(mask[None, :], np.cos(angle), 0.0)
        sine = np.where(mask[None, :], np.where(front[None, :], -np.sin(angle), np.sin(angle)), 0.0)
        return cosine.astype(np.float32), sine.astype(np.float32)

    return tables(rows_total, by_row), tables(GRID_W, ~by_row)


def layer_kernel(
    chips, n_tp, paired,
    q_s_in, kt_in, vt_in, q_l_in, k_l_in, v_l_in, g_qs_in, g_ks_in, g_ql_in, g_kl_in, g_ffn_in, row_in, col_in,
    w_s_in, w_l_in, resid_in, routes_in, route_w_in, w_gate, w_up, w_down, ws_gate_in, ws_up_in, ws_down_in,
    result,
    q_s, kt, vt, q_l, k_l, v_l, g_qs, g_ks, g_ql, g_kl, g_ffn, row_tab, col_tab, w_s, w_l, resid, routes, route_w,
    ws_gate, ws_up, ws_down,
    q_all, kv, m_ref, l_ref, acc, heads, part, got,
    stream_ref, meta, tok, wg, wu, wd, sel, rows_in, outs, res, rs_in, stok, spart, sgot, big, own, cbuf,
    load, rs, rr, ds, dr, xs, xr,
    ms, mr, ts, tr, gs, gr, es, er, bs, br, ss, sr, ps, pr, wsnd, wrcv, fs, fr, ys, yr, wl,
):
    me = lax.axis_index("sp")
    t = lax.axis_index("tp")
    z = me // 2
    c = me % 2
    rows = q_s.shape[0]
    half = rows // 2
    far = chips // 2
    n_tok = resid.shape[0]
    n_small = q_s.shape[1] // 64
    n_large = q_l.shape[1] // LANES

    def at(zz):
        return lax.rem(zz + 2 * chips, chips) * 2 + c

    right, left, mate = at(z + 1), at(z - 1), z * 2 + (1 - c)

    pairs = [
        (kt_in, kt), (vt_in, vt), (k_l_in, k_l), (v_l_in, v_l), (g_ks_in, g_ks), (g_kl_in, g_kl), (row_in, row_tab),
        (col_in, col_tab), (q_s_in, q_s), (q_l_in, q_l), (g_qs_in, g_qs), (g_ql_in, g_ql), (routes_in, routes),
        (route_w_in, route_w), (g_ffn_in, g_ffn), (resid_in, resid), (w_s_in, w_s), (w_l_in, w_l),
        (ws_gate_in, ws_gate), (ws_up_in, ws_up), (ws_down_in, ws_down),
    ]
    loads = [pltpu.make_async_copy(src, dst, load.at[i]) for i, (src, dst) in enumerate(pairs)]
    for one in loads[:16]:
        one.start()
    barrier = pltpu.get_barrier_semaphore()
    for peer in (right, left, mate):
        pl.semaphore_signal(barrier, inc=1, device_id={"sp": peer}, device_id_type=MESH)
    for k in range(1, n_tp):
        pl.semaphore_signal(barrier, inc=1, device_id={"tp": lax.rem(t + k, n_tp)}, device_id_type=MESH)

    odd = lax.rem(lax.axis_index("grp"), 2) if paired else 0
    friend = lax.axis_index("grp") + 1 - 2 * odd
    if paired:
        pl.semaphore_signal(barrier, inc=1, device_id={"grp": friend}, device_id_type=MESH)

    with jax.named_scope("load_a"):
        for one in loads[:8]:
            one.wait()
    lane = lax.broadcasted_iota(jnp.int32, (rows, LANES), 1)
    low = lane < 64
    grid_rows = rows // GRID_W
    first = me * grid_rows

    def table(j):
        pieces = []
        for g in range(grid_rows):
            r = row_tab[first + g][:, j * LANES : (j + 1) * LANES]
            pieces.append(col_tab[:, j * LANES : (j + 1) * LANES] + r)
        return jnp.concatenate(pieces, axis=0)

    def turn(x, j, shift):
        front = lax.rem(lane, 2 * shift) < shift
        other = jnp.where(front, pltpu.roll(x, LANES - shift, 1), pltpu.roll(x, shift, 1))
        return x * table(j) + other * table(j + 1)

    def norm_small(x, gain):
        sq = x * x
        lo = jnp.sum(jnp.where(low, sq, 0.0), axis=1, keepdims=True)
        hi = jnp.sum(jnp.where(low, 0.0, sq), axis=1, keepdims=True)
        scale = jnp.where(low, lax.rsqrt(lo / 64 + norm_eps), lax.rsqrt(hi / 64 + norm_eps))
        return x * scale * gain

    def norm_large(x, gain):
        return x * lax.rsqrt(jnp.mean(x * x, axis=1, keepdims=True) + norm_eps) * gain

    def twice(g):
        return jnp.concatenate([g[...], g[...]], axis=1)

    pair = jnp.concatenate([kt[...].astype(F32).T, vt[...].astype(F32).T], axis=1)
    turned = turn(norm_small(pair, twice(g_ks)), 0, 16)
    kv[me, :, 0:LANES] = jnp.where(low, turned, pair).astype(BF16)
    kv[me, :, LANES : 2 * LANES] = turn(norm_large(k_l[...].astype(F32), g_kl[...]), 2, 32).astype(BF16)
    kv[me, :, 2 * LANES : 3 * LANES] = v_l[...]
    with jax.named_scope("entry"):
        pl.semaphore_wait(barrier, 2 + n_tp + paired)

    def ring(direction, s, h):
        sign = 1 - 2 * direction
        block = at(z - sign * (s - 1))
        span = kv.at[block, pl.ds(h * half, half)]
        return pltpu.make_async_remote_copy(
            src_ref=span, dst_ref=span, send_sem=rs.at[direction, s, h], recv_sem=rr.at[direction, s, h],
            device_id={"sp": right if direction == 0 else left}, device_id_type=MESH,
        )

    def across(direction, s):
        sign = 1 - 2 * direction
        block = at(z - sign * s)
        return pltpu.make_async_remote_copy(
            src_ref=kv.at[block], dst_ref=kv.at[block], send_sem=ds.at[direction, s], recv_sem=dr.at[direction, s],
            device_id={"sp": mate}, device_id_type=MESH,
        )

    for h in range(2):
        ring(0, 1, h).start()
        ring(1, 1, h).start()
    across(0, 0).start()

    holder = c == t // 2
    n_q = 8
    moved = [(w_gate, wg, w_gate.shape[1] // n_q), (w_up, wu, w_up.shape[1] // n_q), (w_down, wd, w_down.shape[1] // n_q)]

    def weight_copy(m, q, k):
        src, dst, span = moved[m]
        aim = lax.rem(t + k, n_tp)
        piece = pl.ds(q * span, span)
        return pltpu.make_async_remote_copy(
            src_ref=src.at[lax.rem(aim, 2), piece], dst_ref=dst.at[t, piece], send_sem=wsnd.at[m, q, k],
            recv_sem=wrcv.at[m, q, k], device_id={"tp": aim}, device_id_type=MESH,
        )

    def weight_in(m, q, k):
        src, dst, span = moved[m]
        piece = pl.ds(q * span, span)
        home = dst.at[lax.rem(t + n_tp - k, n_tp), piece]
        return pltpu.make_async_remote_copy(
            src_ref=home, dst_ref=home, send_sem=wsnd.at[m, q, k],
            recv_sem=wrcv.at[m, q, k], device_id={"tp": lax.rem(t + k, n_tp)}, device_id_type=MESH,
        )

    def weight_on(m, q, k):
        src, dst, span = moved[m]
        piece = pl.ds(q * span, span)
        home = dst.at[lax.rem(t + n_tp - k, n_tp), piece]
        return pltpu.make_async_remote_copy(
            src_ref=home, dst_ref=home, send_sem=fs.at[m, q, k], recv_sem=fr.at[m, q, k],
            device_id={"sp": mate}, device_id_type=MESH,
        )

    def weight_mine(m):
        src, dst, _ = moved[m]
        return pltpu.make_async_copy(src.at[lax.rem(t, 2)], dst.at[t], wl.at[m])

    def weight_to_mate(m):
        src, dst, _ = moved[m]
        return pltpu.make_async_remote_copy(
            src_ref=src.at[lax.rem(t, 2)], dst_ref=dst.at[t], send_sem=fs.at[m, 0, 0], recv_sem=fr.at[m, 0, 0],
            device_id={"sp": mate}, device_id_type=MESH,
        )

    def weight_over(m, q, k):
        src, dst, span = moved[m]
        home = dst.at[lax.rem(t + n_tp - k, n_tp), pl.ds(q * span, span)]
        return pltpu.make_async_remote_copy(
            src_ref=home, dst_ref=home, send_sem=ys.at[m, q, k], recv_sem=yr.at[m, q, k],
            device_id={"grp": friend}, device_id_type=MESH,
        )

    n_own = n_q // 2 if paired else n_q

    def part_own(p):
        return 2 * p + odd if paired else p

    def carry_weights(p):
        q = part_own(p)
        for k in range(1, n_tp):
            @pl.when(c == lax.rem(t + k, n_tp) // 2)
            def _():
                for m in range(3):
                    weight_copy(m, q, k).start()

    def relay_weights(p):
        q = part_own(p)

        @pl.when(holder)
        def _():
            for m in range(3):
                for k in range(1, n_tp):
                    weight_in(m, q, k).wait_recv()
                    weight_on(m, q, k).start()
                    if paired:
                        weight_over(m, q, k).start()

    def relay_other(p):
        q = 2 * p + 1 - odd

        @pl.when(holder)
        def _():
            for m in range(3):
                for k in range(1, n_tp):
                    weight_over(m, q, k).wait_recv()
                    weight_on(m, q, k).start()

    def start_late_loads():
        for one in loads[16:]:
            one.start()

        @pl.when(holder)
        def _():
            for m in range(3):
                weight_mine(m).start()
                weight_to_mate(m).start()

    carry_weights(0)
    carry_weights(1)
    with jax.named_scope("load_b"):
        for one in loads[8:14]:
            one.wait()

    slots = result.shape[0] // 8
    experts = n_tp * chips
    ex = lax.broadcasted_iota(jnp.int32, (experts, n_tok), 0)
    hits = [ex == routes[j : j + 1, :] for j in range(TOPK)]
    named = hits[0]
    for one in hits[1:]:
        named = named | one
    before = lax.broadcasted_iota(jnp.int32, (n_tok, n_tok), 0) < lax.broadcasted_iota(jnp.int32, (n_tok, n_tok), 1)
    ahead = jnp.dot(
        jnp.where(named, 1.0, 0.0).astype(BF16), jnp.where(before, 1.0, 0.0).astype(BF16), preferred_element_type=F32
    )
    meta[z] = jnp.zeros(meta.shape[1:], F32)
    for j in range(TOPK):
        place = jnp.sum(jnp.where(hits[j], ahead, 0.0), axis=0, keepdims=True)
        code = routes[j : j + 1, :].astype(F32) * slots + place
        meta[z, j : j + 1, :] = jnp.concatenate([code, code], axis=1)
    meta[z, 8 : 8 + TOPK, :] = jnp.concatenate([route_w[...], route_w[...]], axis=1)

    for p in range(n_small // 2):
        x = q_s[:, p * LANES : (p + 1) * LANES].astype(F32)
        y = turn(norm_small(x, twice(g_qs)), 0, 16)
        q_all[2 * p] = jnp.where(low, y, 0.0).astype(BF16)
        q_all[2 * p + 1] = jnp.where(low, pltpu.roll(y, 64, 1), 0.0).astype(BF16)
    for p in range(n_large):
        x = q_l[:, p * LANES : (p + 1) * LANES].astype(F32)
        q_all[n_small + p] = turn(norm_large(x, g_ql[...]), 2, 32).astype(BF16)
    m_ref[...] = jnp.full_like(m_ref, far_below)
    l_ref[...] = jnp.zeros_like(l_ref)
    acc[...] = jnp.zeros_like(acc)

    def meta_ring(direction, s):
        sign = 1 - 2 * direction
        block = lax.rem(z - sign * (s - 1) + 2 * chips, chips)
        return pltpu.make_async_remote_copy(
            src_ref=meta.at[block], dst_ref=meta.at[block], send_sem=ms.at[direction, s], recv_sem=mr.at[direction, s],
            device_id={"sp": right if direction == 0 else left}, device_id_type=MESH,
        )

    meta_ring(0, 1).start()
    meta_ring(1, 1).start()

    def absorb(blocks):
        def score(g):
            k_at = 0 if g < n_small else LANES
            keys = jnp.concatenate([kv[b, :, k_at : k_at + LANES] for b in blocks], axis=0)
            return lax.dot_general(q_all[g], keys, (((1,), (1,)), ((), ())), preferred_element_type=F32)

        def mix(g, scores):
            v_at = 0 if g < n_small else 2 * LANES
            factor = (64 if g < n_small else 128) ** -0.5 * LOG2E
            pieces = [scores[:, n : n + LANES] for n in range(0, scores.shape[1], LANES)]
            top = functools.reduce(jnp.maximum, pieces)
            old = m_ref[g]
            new = jnp.maximum(old, jnp.max(top, axis=1, keepdims=True))
            shrink = jnp.exp2((old - new) * factor)
            pieces = [jnp.exp2((one - new) * factor) for one in pieces]
            total = functools.reduce(jnp.add, pieces)
            weights = jnp.concatenate([one.astype(BF16) for one in pieces], axis=1)
            values = jnp.concatenate([kv[b, :, v_at : v_at + LANES] for b in blocks], axis=0)
            m_ref[g] = new
            l_ref[g] = l_ref[g] * shrink + total
            acc[g] = acc[g] * shrink + jnp.dot(weights, values, preferred_element_type=F32)

        ready = score(0)
        for g in range(n_small + n_large):
            scores = ready
            if g + 1 < n_small + n_large:
                ready = score(g + 1)
            mix(g, scores)

    def pass_on(s, h):
        ring(0, s, h).wait_recv()
        ring(0, s + 1, h).start()
        ring(1, s, h).wait_recv()
        ring(1, s + 1, h).start()

    def move(s):
        with jax.named_scope("kv_move"):
            for h in range(2):
                @pl.when(s < far - 1)
                def _():
                    pass_on(s, h)

            @pl.when(s == far - 1)
            def _():
                ring(0, s, 0).wait_recv()
                ring(0, far, 0).start()
                ring(1, s, 0).wait_recv()
                ring(0, s, 1).wait_recv()
                ring(1, s, 1).wait_recv()
                ring(1, far, 1).start()

            @pl.when(s == far)
            def _():
                ring(0, far, 0).wait_recv()
                ring(1, far, 1).wait_recv()

            across(0, s).start()
            meta_ring(0, s).wait_recv()

            @pl.when(s < far)
            def _():
                across(1, s).start()
                meta_ring(1, s).wait_recv()
                meta_ring(0, s + 1).start()

            @pl.when(s < far - 1)
            def _():
                meta_ring(1, s + 1).start()

            @pl.when(s == 2)
            def _():
                start_late_loads()

            for p, when in ((2, 3), (3, 5)):
                @pl.when(s == when)
                def _():
                    carry_weights(p)

            for p, when in ((0, far // 2), (1, far - 2), (2, far)):
                @pl.when(s == when)
                def _():
                    relay_weights(p)


    def other(b):
        return b + 1 - 2 * c

    across(0, 0).wait_recv()

    @pl.loop(0, 2)
    def _(s):
        @pl.when(s == 1)
        def _():
            move(1)

        with jax.named_scope("kv_absorb"):
            absorb([at(z - s), jnp.where(s == 0, other(me), at(z + s))])

    @pl.loop(2, far + 1)
    def _(s):
        move(s)
        across(0, s - 1).wait_recv()
        across(1, s - 1).wait_recv()

        @pl.when(s == far)
        def _():
            across(0, far).wait_recv()

        a, b = at(z - s), at(z + s)
        with jax.named_scope("kv_absorb"):
            absorb([a, jnp.where(s == far, other(a), b), other(at(z - s + 1)), other(at(z + s - 1))])

    with jax.named_scope("load_c"):
        for one in loads[14:18]:
            one.wait()

    def finished(g):
        return acc[g] / jnp.sum(l_ref[g], axis=1, keepdims=True)

    for p in range(n_small // 2):
        both = jnp.where(low, pltpu.roll(finished(2 * p), 64, 1), finished(2 * p + 1))
        heads[:, p * LANES : (p + 1) * LANES] = both.astype(BF16)
    for p in range(n_large):
        heads[:, (n_small // 2 + p) * LANES : (n_small // 2 + p + 1) * LANES] = finished(n_small + p).astype(BF16)

    width = resid.shape[1]
    n_cut = 4
    cut = width // n_cut
    split = n_small * 64

    tok_half = n_tok // 2

    def share(k, h):
        piece = pl.ds(h * tok_half, tok_half)
        return pltpu.make_async_remote_copy(
            src_ref=part.at[lax.rem(t + k, n_tp), piece], dst_ref=got.at[k, piece], send_sem=xs.at[h, k], recv_sem=xr.at[h, k],
            device_id={"tp": lax.rem(t + k, n_tp)}, device_id_type=MESH,
        )

    with jax.named_scope("project"):
        for n in range(n_cut):
            cols = slice(n * cut, (n + 1) * cut)
            whole = jnp.dot(heads[:, :split], w_s[:, cols], preferred_element_type=F32)
            whole = whole + jnp.dot(heads[:, split:], w_l[:, cols], preferred_element_type=F32)
            for d in range(n_tp):
                part[d, :, cols] = whole[d * n_tok : (d + 1) * n_tok].astype(BF16)
    for h in range(2):
        for k in (2, 1, 3):
            share(k, h).start()
    relay_weights(3)

    def share_tokens(k):
        return pltpu.make_async_remote_copy(
            src_ref=stok.at[t], dst_ref=stok.at[t], send_sem=ss.at[k], recv_sem=sr.at[k],
            device_id={"tp": lax.rem(t + k, n_tp)}, device_id_type=MESH,
        )

    def share_back(k):
        return pltpu.make_async_remote_copy(
            src_ref=spart.at[lax.rem(t + k, n_tp)], dst_ref=sgot.at[t], send_sem=ps.at[k], recv_sem=pr.at[k],
            device_id={"tp": lax.rem(t + k, n_tp)}, device_id_type=MESH,
        )

    def zmod(v):
        return lax.rem(v + 2 * chips, chips)

    def token_ring(direction, s, h):
        sign = 1 - 2 * direction
        span = tok.at[zmod(z - sign * (s - 1)), pl.ds(h * tok_half, tok_half)]
        return pltpu.make_async_remote_copy(
            src_ref=span, dst_ref=span, send_sem=ts.at[direction, s, h], recv_sem=tr.at[direction, s, h],
            device_id={"sp": right if direction == 0 else left}, device_id_type=MESH,
        )

    for h in range(2):
        with jax.named_scope("head_sum"):
            piece = slice(h * tok_half, (h + 1) * tok_half)
            total = part[t, piece].astype(F32)
            for k in range(1, n_tp):
                share(k, h).wait_recv()
                total = total + got[k, piece].astype(F32)
            stream = (resid[piece, :].astype(F32) + total).astype(BF16)
            stream_ref[piece, :] = stream
            wide = stream.astype(F32)
            scale = lax.rsqrt(jnp.sum(wide * wide, axis=1, keepdims=True) / width + norm_eps)
            tok[z, piece] = (wide * scale * g_ffn[...]).astype(BF16)
            for direction in range(2):
                token_ring(direction, 1, h).start()
    for p in range(4, n_own):
        carry_weights(p)
    stok[t] = tok[z]
    for k in (2, 1, 3):
        share_tokens(k).start()

    wide_lane = lax.broadcasted_iota(jnp.int32, (8 * slots, LANES), 1)
    wide_row = lax.broadcasted_iota(jnp.int32, (8 * slots, LANES), 0)
    second_token = wide_lane // n_tok
    second_row = lax.rem(wide_row // slots, 2)
    code_row = (z * n_tp + wide_row // (2 * slots)) * slots + lax.rem(wide_row, slots)
    code_row = jnp.where(second_token == second_row, code_row, -1).astype(F32)

    def blocks_of(g):
        last = g == far
        return jnp.where(last, z, zmod(z - g)), zmod(z + g)

    def codes(g):
        a, b = blocks_of(g)
        return jnp.where(lax.broadcasted_iota(jnp.int32, meta.shape[1:], 1) < n_tok, meta[a], meta[b])

    def dispatch(g, k):
        return pltpu.make_async_remote_copy(
            src_ref=sel.at[g - 1, lax.rem(t + k, n_tp)], dst_ref=rows_in.at[g - 1, t], send_sem=gs.at[g, k],
            recv_sem=gr.at[g, k], device_id={"tp": lax.rem(t + k, n_tp)}, device_id_type=MESH,
        )

    def give_back(g, k):
        return pltpu.make_async_remote_copy(
            src_ref=outs.at[g - 1, lax.rem(t + k, n_tp)], dst_ref=res.at[g - 1, t], send_sem=es.at[g, k],
            recv_sem=er.at[g, k], device_id={"tp": lax.rem(t + k, n_tp)}, device_id_type=MESH,
        )

    def pick(g):
        a, b = blocks_of(g)
        code = codes(g)
        chosen = jnp.zeros(wide_row.shape, F32)
        for j in range(TOPK):
            chosen = chosen + jnp.where(code[j : j + 1, :] == code_row, 1.0, 0.0)
        chosen = chosen.astype(BF16)
        both = jnp.concatenate([tok[a], tok[b]], axis=0)
        picked = jnp.dot(chosen, both, preferred_element_type=F32).astype(BF16)
        for i in range(n_tp):
            sel[g - 1, i] = picked[i * 2 * slots : (i + 1) * 2 * slots]
        rows_in[g - 1, t] = sel[g - 1, t]
        for k in (2, 1, 3):
            dispatch(g, k).start()

    def token_step(s):
        for h in range(2):
            @pl.when(s < far - 1)
            def _():
                for d in range(2):
                    token_ring(d, s, h).wait_recv()
                    token_ring(d, s + 1, h).start()

        @pl.when(s == far - 1)
        def _():
            token_ring(0, s, 0).wait_recv()
            token_ring(0, far, 0).start()
            token_ring(1, s, 0).wait_recv()
            token_ring(0, s, 1).wait_recv()
            token_ring(1, s, 1).wait_recv()
            token_ring(1, far, 1).start()

        @pl.when(s == far)
        def _():
            token_ring(0, far, 0).wait_recv()
            token_ring(1, far, 1).wait_recv()

    def weights_in():
        @pl.when(holder)
        def _():
            for m in range(3):
                weight_mine(m).wait()

        @pl.when(jnp.logical_not(holder))
        def _():
            for m in range(3):
                weight_to_mate(m).wait_recv()

                @pl.loop(0, n_q)
                def _(q):
                    for k in range(1, n_tp):
                        weight_on(m, q, k).wait_recv()

    pair_rows = n_tp * 2 * slots

    def expert(first):
        with jax.named_scope("rows_wait"):
            for n in range(2):
                for k in range(1, n_tp):
                    dispatch(first + n, k).wait_recv()
        with jax.named_scope("expert"):
            x = rows_in[pl.ds(first - 1, 2)].reshape(2 * pair_rows, width)
            big[0 : 2 * pair_rows, :] = jnp.zeros((2 * pair_rows, width), F32)

            @pl.loop(0, n_tp)
            def _(j):
                gate = jnp.dot(x, wg[j], preferred_element_type=F32)
                up = jnp.dot(x, wu[j], preferred_element_type=F32)
                hidden = (gate / (1.0 + jnp.exp(-gate)) * up).astype(BF16)
                big[0 : 2 * pair_rows, :] += jnp.dot(hidden, wd[j], preferred_element_type=F32)

            for n in range(2):
                for i in range(n_tp):
                    at_row = n * pair_rows + i * 2 * slots
                    outs[first + n - 1, i] = big[at_row : at_row + 2 * slots, :].astype(BF16)
                res[first + n - 1, t] = outs[first + n - 1, t]

    def return_rows(*groups):
        for g in groups:
            for k in (2, 1, 3):
                give_back(g, k).start()

    @pl.loop(1, far + 1)
    def _(s):
        with jax.named_scope("tok_move"):
            token_step(s)
        with jax.named_scope("pick"):
            pick(s)
        with jax.named_scope("relay"):
            if paired:
                for when, these in ((1, range(3)), (3, (3,))):
                    @pl.when(s == when)
                    def _():
                        for p in these:
                            relay_other(p)
            else:
                @pl.when(s == 4)
                def _():
                    for p in range(4, n_own):
                        relay_weights(p)

        @pl.when(s == 4)
        def _():
            with jax.named_scope("shared"):
                for one in loads[18:]:
                    one.wait()
                for k in range(1, n_tp):
                    share_tokens(k).wait_recv()
                x = stok[...].reshape(n_tp * n_tok, width)
                gate = jnp.dot(x, ws_gate[...], preferred_element_type=F32)
                up = jnp.dot(x, ws_up[...], preferred_element_type=F32)
                hidden = (gate / (1.0 + jnp.exp(-gate)) * up).astype(BF16)
                big[...] = jnp.dot(hidden, ws_down[...], preferred_element_type=F32)
                for d in range(n_tp):
                    spart[d] = big[d * n_tok : (d + 1) * n_tok, :].astype(BF16)
                sgot[t] = spart[t]
                for k in (2, 1, 3):
                    share_back(k).start()

        @pl.when(s == far - 3)
        def _():
            with jax.named_scope("weights_in"):
                weights_in()

        @pl.when((s == far - 3) | (s == far - 2))
        def _():
            expert(2 * (s - (far - 3)) + 1)

    for first in range(5, far, 2):
        expert(first)
    return_rows(*range(far, 0, -1))

    @pl.loop(1, far)
    def _(s):
        for h in range(2):
            token_ring(0, s, h).wait_send()
            token_ring(1, s, h).wait_send()

    token_ring(0, far, 0).wait_send()
    token_ring(1, far, 1).wait_send()

    def sum_ring(direction, i, h):
        piece = pl.ds(h * tok_half, tok_half)
        return pltpu.make_async_remote_copy(
            src_ref=tok.at[direction * far + i - 1, piece], dst_ref=rs_in.at[direction, i - 1, piece],
            send_sem=bs.at[direction, i, h], recv_sem=br.at[direction, i, h],
            device_id={"sp": right if direction == 0 else left}, device_id_type=MESH,
        )

    def weigh(g):
        for k in range(1, n_tp):
            give_back(g, k).wait_recv()
        code = codes(g)
        weight = jnp.zeros(wide_row.shape, F32)
        for j in range(TOPK):
            weight = weight + jnp.where(code[j : j + 1, :] == code_row, code[8 + j : 9 + j, :], 0.0)
        high = weight.astype(BF16)
        rest = weight - high.astype(F32)
        across_rows = jnp.concatenate([high.astype(F32), rest], axis=0).T.astype(BF16)
        back = res[g - 1].reshape(n_tp * 2 * slots, width)
        cbuf[...] = jnp.dot(across_rows, jnp.concatenate([back, back], axis=0), preferred_element_type=F32)

    with jax.named_scope("weigh_first"):
        weigh(far)
    own[...] = cbuf[0:n_tok, :]
    tok[0, 0:tok_half] = cbuf[n_tok : n_tok + tok_half, :].astype(BF16)
    tok[far, tok_half : 2 * tok_half] = cbuf[n_tok + tok_half : 2 * n_tok, :].astype(BF16)
    sum_ring(0, 1, 0).start()
    sum_ring(1, 1, 1).start()

    def send_sum(direction, i, h, add):
        begin = (1 - direction) * n_tok + h * tok_half
        value = cbuf[begin : begin + tok_half, :]
        if add:
            sum_ring(direction, i - 1, h).wait_recv()
            value = value + rs_in[direction, i - 2, h * tok_half : (h + 1) * tok_half].astype(F32)
        tok[direction * far + i - 1, h * tok_half : (h + 1) * tok_half] = value.astype(BF16)
        sum_ring(direction, i, h).start()

    with jax.named_scope("weigh_2"):
        weigh(far - 1)
    send_sum(0, 2, 1, False)
    send_sum(1, 2, 0, False)
    send_sum(0, 2, 0, True)
    send_sum(1, 2, 1, True)

    @pl.loop(3, far + 1)
    def _(i):
        with jax.named_scope("weigh"):
            weigh(far + 1 - i)
        with jax.named_scope("sum"):
            for h in range(2):
                for direction in range(2):
                    send_sum(direction, i, 1 - h if direction == 0 else h, True)

    with jax.named_scope("final"):
        for k in range(1, n_tp):
            share_back(k).wait_recv()
        total = stream_ref[...].astype(F32) + own[...]
        for d in range(n_tp):
            total = total + sgot[d].astype(F32)
        own[...] = total
        for h in range(2):
            piece = slice(h * tok_half, (h + 1) * tok_half)
            for direction in range(2):
                sum_ring(direction, far, h).wait_recv()
            result[piece, :] = (
                own[piece, :] + rs_in[0, far - 1, piece].astype(F32) + rs_in[1, far - 1, piece].astype(F32)
            ).astype(BF16)

    @pl.loop(1, far)
    def _(s):
        for h in range(2):
            ring(0, s, h).wait_send()
            ring(1, s, h).wait_send()
        across(0, s).wait_send()
        across(1, s).wait_send()

    ring(0, far, 0).wait_send()
    ring(1, far, 1).wait_send()
    across(0, 0).wait_send()
    across(0, far).wait_send()
    for h in range(2):
        for k in range(1, n_tp):
            share(k, h).wait_send()

    @pl.loop(2, far + 1)
    def _(i):
        for h in range(2):
            for d in range(2):
                sum_ring(d, i, h).wait_send()

    sum_ring(0, 1, 0).wait_send()
    sum_ring(1, 1, 1).wait_send()
    for k in range(1, n_tp):
        share_tokens(k).wait_send()
        share_back(k).wait_send()

        @pl.loop(1, far + 1)
        def _(g):
            dispatch(g, k).wait_send()
            give_back(g, k).wait_send()

        @pl.when(c == lax.rem(t + k, n_tp) // 2)
        def _():
            @pl.loop(0, n_own)
            def _(p):
                for m in range(3):
                    weight_copy(m, part_own(p), k).wait_send()

    @pl.when(holder)
    def _():
        for m in range(3):
            weight_to_mate(m).wait_send()

            @pl.loop(0, n_q)
            def _(q):
                for k in range(1, n_tp):
                    weight_on(m, q, k).wait_send()

            if paired:
                @pl.loop(0, n_own)
                def _(p):
                    for k in range(1, n_tp):
                        weight_over(m, part_own(p), k).wait_send()

    @pl.loop(1, far + 1)
    def _(s):
        meta_ring(0, s).wait_send()

    @pl.loop(1, far)
    def _(s):
        meta_ring(1, s).wait_send()


def layer(
    residual_in, q_small, k_small, v_small, q_large, k_large, v_large, gain_qs, gain_ks, gain_ql, gain_kl,
    w_out_small, w_out_large, g_ffn, routes, route_w, w_gate, w_up, w_down, ws_gate, ws_up, ws_down,
):
    n_sp, n_tp = lax.axis_size("sp"), lax.axis_size("tp")
    chips = n_sp // 2
    paired = lax.axis_size("grp") % 2 == 0
    far = chips // 2
    rows = q_small.shape[0]
    rows_total = n_sp * rows // GRID_W
    tok, width = residual_in.shape
    groups = q_small.shape[1] // 64 + q_large.shape[1] // LANES
    slots = max(2, 2 * tok * TOPK // (w_gate.shape[0] * n_sp))
    assert w_gate.shape[0] * 2 == n_tp and 2 * tok == LANES and slots == 8
    (rc_s, rs_s), (cc_s, cs_s) = angle_tables(64, rows_total)
    (rc_l, rs_l), (cc_l, cs_l) = angle_tables(128, rows_total)
    row_tab = jnp.asarray(np.concatenate([rc_s, rs_s, rc_l, rs_l], axis=1)[:, None, :])
    col_tab = jnp.asarray(np.concatenate([cc_s, cs_s, cc_l, cs_l], axis=1))
    operands = [
        q_small, k_small.T, v_small.T, q_large, k_large, v_large, gain_qs.reshape(1, -1), gain_ks.reshape(1, -1),
        gain_ql.reshape(1, -1), gain_kl.reshape(1, -1), g_ffn.reshape(1, -1), row_tab, col_tab, w_out_small, w_out_large,
        residual_in, routes.T, route_w.T, w_gate, w_up, w_down, ws_gate, ws_up, ws_down,
    ]
    n_q = 8
    dma = pltpu.SemaphoreType.DMA
    copies = [pltpu.VMEM(x.shape, x.dtype) for x in operands[:18] + operands[21:]]

    def bf(*shape):
        return pltpu.VMEM(shape, BF16)

    def f32(*shape):
        return pltpu.VMEM(shape, F32)

    moved_rows = (far, n_tp, 2 * slots, width)
    return pl.pallas_call(
        functools.partial(layer_kernel, chips, n_tp, paired),
        out_shape=jax.ShapeDtypeStruct((tok, width), BF16),
        in_specs=[pl.BlockSpec(memory_space=pl.ANY)] * len(operands),
        out_specs=pl.BlockSpec(memory_space=pltpu.VMEM),
        scratch_shapes=copies + [
            bf(groups, rows, LANES), bf(n_sp, rows, 3 * LANES), f32(groups, rows, LANES), f32(groups, rows, LANES),
            f32(groups, rows, LANES), bf(rows, q_small.shape[1] + q_large.shape[1]),
            bf(n_tp, tok, width), bf(n_tp, tok, width),
            bf(tok, width), f32(chips, 16, LANES), bf(chips, tok, width),
            bf(n_tp, *w_gate.shape[1:]), bf(n_tp, *w_up.shape[1:]), bf(n_tp, *w_down.shape[1:]),
            bf(*moved_rows), bf(*moved_rows), bf(*moved_rows), bf(*moved_rows), bf(2, far, tok, width),
            bf(n_tp, tok, width), bf(n_tp, tok, width), bf(n_tp, tok, width),
            f32(n_tp * tok, width), f32(tok, width), f32(2 * tok, width),
            dma((len(copies),)),
            dma((2, far + 1, 2)), dma((2, far + 1, 2)), dma((2, far + 1)), dma((2, far + 1)), dma((2, n_tp)), dma((2, n_tp)),
            dma((2, far + 1)), dma((2, far + 1)), dma((2, far + 1, 2)), dma((2, far + 1, 2)),
            dma((far + 1, n_tp)), dma((far + 1, n_tp)), dma((far + 1, n_tp)), dma((far + 1, n_tp)),
            dma((2, far + 1, 2)), dma((2, far + 1, 2)), dma((n_tp,)), dma((n_tp,)), dma((n_tp,)), dma((n_tp,)),
            *[dma((3, n_q, n_tp))] * 6, dma((3,)),
        ],
        compiler_params=pltpu.CompilerParams(collective_id=0, has_side_effects=True, vmem_limit_bytes=67_043_328),
        name="layer",
    )(*operands)


def solution(mesh):
    part = P(("grp", "sp"), "tp")
    each = P(("grp", "sp", "tp"), None)
    placed = (
        each, part, part, part, part, part, part, P(), P(), P(), P(), P("tp", None), P("tp", None), P(), each, each,
        P("sp", None, "tp"), P("sp", None, "tp"), P("sp", "tp", None), P(None, "tp"), P(None, "tp"), P("tp", None),
    )
    return jax.shard_map(layer, mesh=mesh, in_specs=placed, out_specs=each, check_vma=False)
```

```python
import functools
import math

import jax
import jax.numpy as jnp
import numpy as np
from jax import lax
from jax.experimental import pallas as pl
from jax.experimental.pallas import tpu as pltpu
from jax.sharding import PartitionSpec as P

GRID_W = 64
TOPK = 4
norm_eps = 1e-06
rope_base = 10000.0
far_below = -1e30
LANES = 128
LOG2E = math.log2(math.e)
MESH = pl.DeviceIdType.MESH
F32 = jnp.float32
BF16 = jnp.bfloat16


def angle_tables(channels, rows_total):
    quarter = channels // 4
    lane = np.arange(LANES) % channels
    by_row = lane < channels // 2
    front = lane % (channels // 2) < quarter
    inverse = (1.0 / rope_base ** (np.arange(quarter, dtype=np.float32) / np.float32(quarter))).astype(np.float32)
    freq = inverse[lane % quarter]

    def tables(count, mask):
        angle = np.arange(count, dtype=np.float32)[:, None] * freq[None, :]
        angle = angle.astype(np.float32).astype(np.float64)
        cosine = np.where(mask[None, :], np.cos(angle), 0.0)
        sine = np.where(mask[None, :], np.where(front[None, :], -np.sin(angle), np.sin(angle)), 0.0)
        return cosine.astype(np.float32), sine.astype(np.float32)

    return tables(rows_total, by_row), tables(GRID_W, ~by_row)


def layer_kernel(
    chips, n_tp, paired,
    q_s_in, kt_in, vt_in, q_l_in, k_l_in, v_l_in, g_qs_in, g_ks_in, g_ql_in, g_kl_in, g_ffn_in, row_in, col_in,
    w_s_in, w_l_in, resid_in, routes_in, route_w_in, w_gate, w_up, w_down, ws_gate_in, ws_up_in, ws_down_in,
    result,
    q_s, kt, vt, q_l, k_l, v_l, g_qs, g_ks, g_ql, g_kl, g_ffn, row_tab, col_tab, w_s, w_l, resid, routes, route_w,
    ws_gate, ws_up, ws_down,
    q_all, kv, m_ref, l_ref, acc, heads, part, got,
    stream_ref, meta, tok, wg, wu, wd, sel, rows_in, outs, res, rs_in, stok, spart, sgot, big, own, cbuf,
    load, rs, rr, ds, dr, xs, xr,
    ms, mr, ts, tr, gs, gr, es, er, bs, br, ss, sr, ps, pr, wsnd, wrcv, fs, fr, ys, yr, wl,
):
    me = lax.axis_index("sp")
    t = lax.axis_index("tp")
    z = me // 2
    c = me % 2
    rows = q_s.shape[0]
    half = rows // 2
    far = chips // 2
    n_tok = resid.shape[0]
    n_small = q_s.shape[1] // 64
    n_large = q_l.shape[1] // LANES

    def at(zz):
        return lax.rem(zz + 2 * chips, chips) * 2 + c

    right, left, mate = at(z + 1), at(z - 1), z * 2 + (1 - c)

    pairs = [
        (kt_in, kt), (vt_in, vt), (k_l_in, k_l), (v_l_in, v_l), (g_ks_in, g_ks), (g_kl_in, g_kl), (row_in, row_tab),
        (col_in, col_tab), (q_s_in, q_s), (q_l_in, q_l), (g_qs_in, g_qs), (g_ql_in, g_ql), (routes_in, routes),
        (route_w_in, route_w), (g_ffn_in, g_ffn), (resid_in, resid), (w_s_in, w_s), (w_l_in, w_l),
        (ws_gate_in, ws_gate), (ws_up_in, ws_up), (ws_down_in, ws_down),
    ]
    loads = [pltpu.make_async_copy(src, dst, load.at[i]) for i, (src, dst) in enumerate(pairs)]
    for one in loads[:16]:
        one.start()
    barrier = pltpu.get_barrier_semaphore()
    for peer in (right, left, mate):
        pl.semaphore_signal(barrier, inc=1, device_id={"sp": peer}, device_id_type=MESH)
    for k in range(1, n_tp):
        pl.semaphore_signal(barrier, inc=1, device_id={"tp": lax.rem(t + k, n_tp)}, device_id_type=MESH)

    odd = lax.rem(lax.axis_index("grp"), 2) if paired else 0
    friend = lax.axis_index("grp") + 1 - 2 * odd
    if paired:
        pl.semaphore_signal(barrier, inc=1, device_id={"grp": friend}, device_id_type=MESH)

    with jax.named_scope("load_a"):
        for one in loads[:8]:
            one.wait()
    lane = lax.broadcasted_iota(jnp.int32, (rows, LANES), 1)
    low = lane < 64
    grid_rows = rows // GRID_W
    first = me * grid_rows

    def table(j):
        pieces = []
        for g in range(grid_rows):
            r = row_tab[first + g][:, j * LANES : (j + 1) * LANES]
            pieces.append(col_tab[:, j * LANES : (j + 1) * LANES] + r)
        return jnp.concatenate(pieces, axis=0)

    def turn(x, j, shift):
        front = lax.rem(lane, 2 * shift) < shift
        other = jnp.where(front, pltpu.roll(x, LANES - shift, 1), pltpu.roll(x, shift, 1))
        return x * table(j) + other * table(j + 1)

    def norm_small(x, gain):
        sq = x * x
        lo = jnp.sum(jnp.where(low, sq, 0.0), axis=1, keepdims=True)
        hi = jnp.sum(jnp.where(low, 0.0, sq), axis=1, keepdims=True)
        scale = jnp.where(low, lax.rsqrt(lo / 64 + norm_eps), lax.rsqrt(hi / 64 + norm_eps))
        return x * scale * gain

    def norm_large(x, gain):
        return x * lax.rsqrt(jnp.mean(x * x, axis=1, keepdims=True) + norm_eps) * gain

    def twice(g):
        return jnp.concatenate([g[...], g[...]], axis=1)

    pair = jnp.concatenate([kt[...].astype(F32).T, vt[...].astype(F32).T], axis=1)
    turned = turn(norm_small(pair, twice(g_ks)), 0, 16)
    kv[me, :, 0:LANES] = jnp.where(low, turned, pair).astype(BF16)
    kv[me, :, LANES : 2 * LANES] = turn(norm_large(k_l[...].astype(F32), g_kl[...]), 2, 32).astype(BF16)
    kv[me, :, 2 * LANES : 3 * LANES] = v_l[...]
    with jax.named_scope("entry"):
        pl.semaphore_wait(barrier, 2 + n_tp + paired)

    def ring(direction, s, h):
        sign = 1 - 2 * direction
        block = at(z - sign * (s - 1))
        span = kv.at[block, pl.ds(h * half, half)]
        return pltpu.make_async_remote_copy(
            src_ref=span, dst_ref=span, send_sem=rs.at[direction, s, h], recv_sem=rr.at[direction, s, h],
            device_id={"sp": right if direction == 0 else left}, device_id_type=MESH,
        )

    def across(direction, s):
        sign = 1 - 2 * direction
        block = at(z - sign * s)
        return pltpu.make_async_remote_copy(
            src_ref=kv.at[block], dst_ref=kv.at[block], send_sem=ds.at[direction, s], recv_sem=dr.at[direction, s],
            device_id={"sp": mate}, device_id_type=MESH,
        )

    for h in range(2):
        ring(0, 1, h).start()
        ring(1, 1, h).start()
    across(0, 0).start()

    holder = c == t // 2
    n_q = 8
    moved = [(w_gate, wg, w_gate.shape[1] // n_q), (w_up, wu, w_up.shape[1] // n_q), (w_down, wd, w_down.shape[1] // n_q)]

    def weight_copy(m, q, k):
        src, dst, span = moved[m]
        aim = lax.rem(t + k, n_tp)
        piece = pl.ds(q * span, span)
        return pltpu.make_async_remote_copy(
            src_ref=src.at[lax.rem(aim, 2), piece], dst_ref=dst.at[t, piece], send_sem=wsnd.at[m, q, k],
            recv_sem=wrcv.at[m, q, k], device_id={"tp": aim}, device_id_type=MESH,
        )

    def weight_in(m, q, k):
        src, dst, span = moved[m]
        piece = pl.ds(q * span, span)
        home = dst.at[lax.rem(t + n_tp - k, n_tp), piece]
        return pltpu.make_async_remote_copy(
            src_ref=home, dst_ref=home, send_sem=wsnd.at[m, q, k],
            recv_sem=wrcv.at[m, q, k], device_id={"tp": lax.rem(t + k, n_tp)}, device_id_type=MESH,
        )

    def weight_on(m, q, k):
        src, dst, span = moved[m]
        piece = pl.ds(q * span, span)
        home = dst.at[lax.rem(t + n_tp - k, n_tp), piece]
        return pltpu.make_async_remote_copy(
            src_ref=home, dst_ref=home, send_sem=fs.at[m, q, k], recv_sem=fr.at[m, q, k],
            device_id={"sp": mate}, device_id_type=MESH,
        )

    def weight_mine(m):
        src, dst, _ = moved[m]
        return pltpu.make_async_copy(src.at[lax.rem(t, 2)], dst.at[t], wl.at[m])

    def weight_to_mate(m):
        src, dst, _ = moved[m]
        return pltpu.make_async_remote_copy(
            src_ref=src.at[lax.rem(t, 2)], dst_ref=dst.at[t], send_sem=fs.at[m, 0, 0], recv_sem=fr.at[m, 0, 0],
            device_id={"sp": mate}, device_id_type=MESH,
        )

    def weight_over(m, q, k):
        src, dst, span = moved[m]
        home = dst.at[lax.rem(t + n_tp - k, n_tp), pl.ds(q * span, span)]
        return pltpu.make_async_remote_copy(
            src_ref=home, dst_ref=home, send_sem=ys.at[m, q, k], recv_sem=yr.at[m, q, k],
            device_id={"grp": friend}, device_id_type=MESH,
        )

    n_own = n_q // 2 if paired else n_q

    def part_own(p):
        return 2 * p + odd if paired else p

    def carry_weights(p):
        q = part_own(p)
        for k in range(1, n_tp):
            @pl.when(c == lax.rem(t + k, n_tp) // 2)
            def _():
                for m in range(3):
                    weight_copy(m, q, k).start()

    def relay_weights(p):
        q = part_own(p)

        @pl.when(holder)
        def _():
            for m in range(3):
                for k in range(1, n_tp):
                    weight_in(m, q, k).wait_recv()
                    weight_on(m, q, k).start()
                    if paired:
                        weight_over(m, q, k).start()

    def relay_other(p):
        q = 2 * p + 1 - odd

        @pl.when(holder)
        def _():
            for m in range(3):
                for k in range(1, n_tp):
                    weight_over(m, q, k).wait_recv()
                    weight_on(m, q, k).start()

    def start_late_loads():
        for one in loads[16:]:
            one.start()

        @pl.when(holder)
        def _():
            for m in range(3):
                weight_mine(m).start()
                weight_to_mate(m).start()

    carry_weights(0)
    carry_weights(1)
    with jax.named_scope("load_b"):
        for one in loads[8:14]:
            one.wait()

    slots = result.shape[0] // 8
    experts = n_tp * chips
    ex = lax.broadcasted_iota(jnp.int32, (experts, n_tok), 0)
    hits = [ex == routes[j : j + 1, :] for j in range(TOPK)]
    named = hits[0]
    for one in hits[1:]:
        named = named | one
    before = lax.broadcasted_iota(jnp.int32, (n_tok, n_tok), 0) < lax.broadcasted_iota(jnp.int32, (n_tok, n_tok), 1)
    ahead = jnp.dot(
        jnp.where(named, 1.0, 0.0).astype(BF16), jnp.where(before, 1.0, 0.0).astype(BF16), preferred_element_type=F32
    )
    meta[z] = jnp.zeros(meta.shape[1:], F32)
    for j in range(TOPK):
        place = jnp.sum(jnp.where(hits[j], ahead, 0.0), axis=0, keepdims=True)
        code = routes[j : j + 1, :].astype(F32) * slots + place
        meta[z, j : j + 1, :] = jnp.concatenate([code, code], axis=1)
    meta[z, 8 : 8 + TOPK, :] = jnp.concatenate([route_w[...], route_w[...]], axis=1)

    for p in range(n_small // 2):
        x = q_s[:, p * LANES : (p + 1) * LANES].astype(F32)
        y = turn(norm_small(x, twice(g_qs)), 0, 16)
        q_all[2 * p] = jnp.where(low, y, 0.0).astype(BF16)
        q_all[2 * p + 1] = jnp.where(low, pltpu.roll(y, 64, 1), 0.0).astype(BF16)
    for p in range(n_large):
        x = q_l[:, p * LANES : (p + 1) * LANES].astype(F32)
        q_all[n_small + p] = turn(norm_large(x, g_ql[...]), 2, 32).astype(BF16)
    m_ref[...] = jnp.full_like(m_ref, far_below)
    l_ref[...] = jnp.zeros_like(l_ref)
    acc[...] = jnp.zeros_like(acc)

    def meta_ring(direction, s):
        sign = 1 - 2 * direction
        block = lax.rem(z - sign * (s - 1) + 2 * chips, chips)
        return pltpu.make_async_remote_copy(
            src_ref=meta.at[block], dst_ref=meta.at[block], send_sem=ms.at[direction, s], recv_sem=mr.at[direction, s],
            device_id={"sp": right if direction == 0 else left}, device_id_type=MESH,
        )

    meta_ring(0, 1).start()
    meta_ring(1, 1).start()

    def absorb(blocks):
        def score(g):
            k_at = 0 if g < n_small else LANES
            keys = jnp.concatenate([kv[b, :, k_at : k_at + LANES] for b in blocks], axis=0)
            return lax.dot_general(q_all[g], keys, (((1,), (1,)), ((), ())), preferred_element_type=F32)

        def mix(g, scores):
            v_at = 0 if g < n_small else 2 * LANES
            factor = (64 if g < n_small else 128) ** -0.5 * LOG2E
            pieces = [scores[:, n : n + LANES] for n in range(0, scores.shape[1], LANES)]
            top = functools.reduce(jnp.maximum, pieces)
            old = m_ref[g]
            new = jnp.maximum(old, jnp.max(top, axis=1, keepdims=True))
            shrink = jnp.exp2((old - new) * factor)
            pieces = [jnp.exp2((one - new) * factor) for one in pieces]
            total = functools.reduce(jnp.add, pieces)
            weights = jnp.concatenate([one.astype(BF16) for one in pieces], axis=1)
            values = jnp.concatenate([kv[b, :, v_at : v_at + LANES] for b in blocks], axis=0)
            m_ref[g] = new
            l_ref[g] = l_ref[g] * shrink + total
            acc[g] = acc[g] * shrink + jnp.dot(weights, values, preferred_element_type=F32)

        ready = score(0)
        for g in range(n_small + n_large):
            scores = ready
            if g + 1 < n_small + n_large:
                ready = score(g + 1)
            mix(g, scores)

    def pass_on(s, h):
        ring(0, s, h).wait_recv()
        ring(0, s + 1, h).start()
        ring(1, s, h).wait_recv()
        ring(1, s + 1, h).start()

    def move(s):
        with jax.named_scope("kv_move"):
            for h in range(2):
                @pl.when(s < far - 1)
                def _():
                    pass_on(s, h)

            @pl.when(s == far - 1)
            def _():
                ring(0, s, 0).wait_recv()
                ring(0, far, 0).start()
                ring(1, s, 0).wait_recv()
                ring(0, s, 1).wait_recv()
                ring(1, s, 1).wait_recv()
                ring(1, far, 1).start()

            @pl.when(s == far)
            def _():
                ring(0, far, 0).wait_recv()
                ring(1, far, 1).wait_recv()

            across(0, s).start()
            meta_ring(0, s).wait_recv()

            @pl.when(s < far)
            def _():
                across(1, s).start()
                meta_ring(1, s).wait_recv()
                meta_ring(0, s + 1).start()

            @pl.when(s < far - 1)
            def _():
                meta_ring(1, s + 1).start()

            @pl.when(s == 2)
            def _():
                start_late_loads()

            for p, when in ((2, 3), (3, 5)):
                @pl.when(s == when)
                def _():
                    carry_weights(p)

            for p, when in ((0, far // 2), (1, far - 2), (2, far)):
                @pl.when(s == when)
                def _():
                    relay_weights(p)


    def other(b):
        return b + 1 - 2 * c

    across(0, 0).wait_recv()

    @pl.loop(0, 2)
    def _(s):
        @pl.when(s == 1)
        def _():
            move(1)

        with jax.named_scope("kv_absorb"):
            absorb([at(z - s), jnp.where(s == 0, other(me), at(z + s))])

    @pl.loop(2, far + 1)
    def _(s):
        move(s)
        across(0, s - 1).wait_recv()
        across(1, s - 1).wait_recv()

        @pl.when(s == far)
        def _():
            across(0, far).wait_recv()

        a, b = at(z - s), at(z + s)
        with jax.named_scope("kv_absorb"):
            absorb([a, jnp.where(s == far, other(a), b), other(at(z - s + 1)), other(at(z + s - 1))])

    with jax.named_scope("load_c"):
        for one in loads[14:18]:
            one.wait()

    def finished(g):
        return acc[g] / jnp.sum(l_ref[g], axis=1, keepdims=True)

    for p in range(n_small // 2):
        both = jnp.where(low, pltpu.roll(finished(2 * p), 64, 1), finished(2 * p + 1))
        heads[:, p * LANES : (p + 1) * LANES] = both.astype(BF16)
    for p in range(n_large):
        heads[:, (n_small // 2 + p) * LANES : (n_small // 2 + p + 1) * LANES] = finished(n_small + p).astype(BF16)

    width = resid.shape[1]
    n_cut = 4
    cut = width // n_cut
    split = n_small * 64

    tok_half = n_tok // 2
    n_part = 4
    tok_part = n_tok // n_part

    def share(k, h):
        piece = pl.ds(h * tok_part, tok_part)
        return pltpu.make_async_remote_copy(
            src_ref=part.at[lax.rem(t + k, n_tp), piece], dst_ref=got.at[k, piece], send_sem=xs.at[h, k], recv_sem=xr.at[h, k],
            device_id={"tp": lax.rem(t + k, n_tp)}, device_id_type=MESH,
        )

    with jax.named_scope("project"):
        for n in range(n_cut):
            cols = slice(n * cut, (n + 1) * cut)
            whole = jnp.dot(heads[:, :split], w_s[:, cols], preferred_element_type=F32)
            whole = whole + jnp.dot(heads[:, split:], w_l[:, cols], preferred_element_type=F32)
            for d in range(n_tp):
                part[d, :, cols] = whole[d * n_tok : (d + 1) * n_tok].astype(BF16)
    for h in range(n_part):
        for k in (2, 1, 3):
            share(k, h).start()
    relay_weights(3)

    def share_tokens(k):
        return pltpu.make_async_remote_copy(
            src_ref=stok.at[t], dst_ref=stok.at[t], send_sem=ss.at[k], recv_sem=sr.at[k],
            device_id={"tp": lax.rem(t + k, n_tp)}, device_id_type=MESH,
        )

    def share_back(k):
        return pltpu.make_async_remote_copy(
            src_ref=spart.at[lax.rem(t + k, n_tp)], dst_ref=sgot.at[t], send_sem=ps.at[k], recv_sem=pr.at[k],
            device_id={"tp": lax.rem(t + k, n_tp)}, device_id_type=MESH,
        )

    def zmod(v):
        return lax.rem(v + 2 * chips, chips)

    def token_ring(direction, s, h):
        sign = 1 - 2 * direction
        span = tok.at[zmod(z - sign * (s - 1)), pl.ds(h * tok_part, tok_part)]
        return pltpu.make_async_remote_copy(
            src_ref=span, dst_ref=span, send_sem=ts.at[direction, s, h], recv_sem=tr.at[direction, s, h],
            device_id={"sp": right if direction == 0 else left}, device_id_type=MESH,
        )

    for h in range(n_part):
        with jax.named_scope("head_sum"):
            piece = slice(h * tok_part, (h + 1) * tok_part)
            total = part[t, piece].astype(F32)
            for k in range(1, n_tp):
                share(k, h).wait_recv()
                total = total + got[k, piece].astype(F32)
            stream = (resid[piece, :].astype(F32) + total).astype(BF16)
            stream_ref[piece, :] = stream
            wide = stream.astype(F32)
            scale = lax.rsqrt(jnp.sum(wide * wide, axis=1, keepdims=True) / width + norm_eps)
            tok[z, piece] = (wide * scale * g_ffn[...]).astype(BF16)
            for direction in range(2):
                token_ring(direction, 1, h).start()
    for p in range(4, n_own):
        carry_weights(p)
    stok[t] = tok[z]
    for k in (2, 1, 3):
        share_tokens(k).start()

    wide_lane = lax.broadcasted_iota(jnp.int32, (8 * slots, LANES), 1)
    wide_row = lax.broadcasted_iota(jnp.int32, (8 * slots, LANES), 0)
    second_token = wide_lane // n_tok
    second_row = lax.rem(wide_row // slots, 2)
    code_row = (z * n_tp + wide_row // (2 * slots)) * slots + lax.rem(wide_row, slots)
    code_row = jnp.where(second_token == second_row, code_row, -1).astype(F32)

    def blocks_of(g):
        last = g == far
        return jnp.where(last, z, zmod(z - g)), zmod(z + g)

    def codes(g):
        a, b = blocks_of(g)
        return jnp.where(lax.broadcasted_iota(jnp.int32, meta.shape[1:], 1) < n_tok, meta[a], meta[b])

    def dispatch(g, k):
        return pltpu.make_async_remote_copy(
            src_ref=sel.at[g - 1, lax.rem(t + k, n_tp)], dst_ref=rows_in.at[g - 1, t], send_sem=gs.at[g, k],
            recv_sem=gr.at[g, k], device_id={"tp": lax.rem(t + k, n_tp)}, device_id_type=MESH,
        )

    def give_back(g, k):
        return pltpu.make_async_remote_copy(
            src_ref=outs.at[g - 1, lax.rem(t + k, n_tp)], dst_ref=res.at[g - 1, t], send_sem=es.at[g, k],
            recv_sem=er.at[g, k], device_id={"tp": lax.rem(t + k, n_tp)}, device_id_type=MESH,
        )

    def pick(g):
        a, b = blocks_of(g)
        code = codes(g)
        chosen = jnp.zeros(wide_row.shape, F32)
        for j in range(TOPK):
            chosen = chosen + jnp.where(code[j : j + 1, :] == code_row, 1.0, 0.0)
        chosen = chosen.astype(BF16)
        both = jnp.concatenate([tok[a], tok[b]], axis=0)
        picked = jnp.dot(chosen, both, preferred_element_type=F32).astype(BF16)
        for i in range(n_tp):
            sel[g - 1, i] = picked[i * 2 * slots : (i + 1) * 2 * slots]
        rows_in[g - 1, t] = sel[g - 1, t]
        for k in (2, 1, 3):
            dispatch(g, k).start()

    def takes_far(direction, h):
        return (h < n_part // 2) == (direction == 0)

    def token_step(s):
        for h in range(n_part):
            for d in range(2):
                @pl.when(s < far if not takes_far(d, h) else s <= far)
                def _():
                    token_ring(d, s, h).wait_recv()

                @pl.when(s < far - 1 if not takes_far(d, h) else s < far)
                def _():
                    token_ring(d, s + 1, h).start()

    def weights_in():
        @pl.when(holder)
        def _():
            for m in range(3):
                weight_mine(m).wait()

        @pl.when(jnp.logical_not(holder))
        def _():
            for m in range(3):
                weight_to_mate(m).wait_recv()

                @pl.loop(0, n_q)
                def _(q):
                    for k in range(1, n_tp):
                        weight_on(m, q, k).wait_recv()

    pair_rows = n_tp * 2 * slots

    def expert(first):
        with jax.named_scope("rows_wait"):
            for n in range(2):
                for k in range(1, n_tp):
                    dispatch(first + n, k).wait_recv()
        with jax.named_scope("expert"):
            x = rows_in[pl.ds(first - 1, 2)].reshape(2 * pair_rows, width)
            big[0 : 2 * pair_rows, :] = jnp.zeros((2 * pair_rows, width), F32)

            @pl.loop(0, n_tp)
            def _(j):
                gate = jnp.dot(x, wg[j], preferred_element_type=F32)
                up = jnp.dot(x, wu[j], preferred_element_type=F32)
                hidden = (gate / (1.0 + jnp.exp(-gate)) * up).astype(BF16)
                big[0 : 2 * pair_rows, :] += jnp.dot(hidden, wd[j], preferred_element_type=F32)

            for n in range(2):
                for i in range(n_tp):
                    at_row = n * pair_rows + i * 2 * slots
                    outs[first + n - 1, i] = big[at_row : at_row + 2 * slots, :].astype(BF16)
                res[first + n - 1, t] = outs[first + n - 1, t]

    def return_rows(*groups):
        for g in groups:
            for k in (2, 1, 3):
                give_back(g, k).start()

    @pl.loop(1, far + 1)
    def _(s):
        with jax.named_scope("tok_move"):
            token_step(s)
        with jax.named_scope("pick"):
            pick(s)
        with jax.named_scope("relay"):
            if paired:
                for when, these in ((1, range(3)), (3, (3,))):
                    @pl.when(s == when)
                    def _():
                        for p in these:
                            relay_other(p)
            else:
                @pl.when(s == 4)
                def _():
                    for p in range(4, n_own):
                        relay_weights(p)

        @pl.when(s == 4)
        def _():
            with jax.named_scope("shared"):
                for one in loads[18:]:
                    one.wait()
                for k in range(1, n_tp):
                    share_tokens(k).wait_recv()
                x = stok[...].reshape(n_tp * n_tok, width)
                gate = jnp.dot(x, ws_gate[...], preferred_element_type=F32)
                up = jnp.dot(x, ws_up[...], preferred_element_type=F32)
                hidden = (gate / (1.0 + jnp.exp(-gate)) * up).astype(BF16)
                big[...] = jnp.dot(hidden, ws_down[...], preferred_element_type=F32)
                for d in range(n_tp):
                    spart[d] = big[d * n_tok : (d + 1) * n_tok, :].astype(BF16)
                sgot[t] = spart[t]

        @pl.when(s == far - 3)
        def _():
            with jax.named_scope("weights_in"):
                weights_in()

        @pl.when((s >= far - 3) & (s != far - 1))
        def _():
            expert(jnp.where(s == far, far - 3, 2 * (s - (far - 3)) + 1))

    expert(far - 1)
    return_rows(*range(far, 2, -1))
    for k in (2, 1, 3):
        share_back(k).start()
    return_rows(2, 1)

    @pl.loop(1, far)
    def _(s):
        for h in range(n_part):
            token_ring(0, s, h).wait_send()
            token_ring(1, s, h).wait_send()

    for h in range(n_part):
        token_ring(0 if takes_far(0, h) else 1, far, h).wait_send()

    def sum_ring(direction, i, h):
        piece = pl.ds(h * tok_half, tok_half)
        return pltpu.make_async_remote_copy(
            src_ref=tok.at[direction * far + i - 1, piece], dst_ref=rs_in.at[direction, i - 1, piece],
            send_sem=bs.at[direction, i, h], recv_sem=br.at[direction, i, h],
            device_id={"sp": right if direction == 0 else left}, device_id_type=MESH,
        )

    def weigh(g):
        for k in range(1, n_tp):
            give_back(g, k).wait_recv()
        code = codes(g)
        weight = jnp.zeros(wide_row.shape, F32)
        for j in range(TOPK):
            weight = weight + jnp.where(code[j : j + 1, :] == code_row, code[8 + j : 9 + j, :], 0.0)
        high = weight.astype(BF16)
        rest = weight - high.astype(F32)
        across_rows = jnp.concatenate([high.astype(F32), rest], axis=0).T.astype(BF16)
        back = res[g - 1].reshape(n_tp * 2 * slots, width)
        cbuf[...] = jnp.dot(across_rows, jnp.concatenate([back, back], axis=0), preferred_element_type=F32)

    with jax.named_scope("weigh_first"):
        weigh(far)
    own[...] = cbuf[0:n_tok, :]
    tok[0, 0:tok_half] = cbuf[n_tok : n_tok + tok_half, :].astype(BF16)
    tok[far, tok_half : 2 * tok_half] = cbuf[n_tok + tok_half : 2 * n_tok, :].astype(BF16)
    sum_ring(0, 1, 0).start()
    sum_ring(1, 1, 1).start()

    def send_sum(direction, i, h, add):
        begin = (1 - direction) * n_tok + h * tok_half
        value = cbuf[begin : begin + tok_half, :]
        if add:
            sum_ring(direction, i - 1, h).wait_recv()
            value = value + rs_in[direction, i - 2, h * tok_half : (h + 1) * tok_half].astype(F32)
        tok[direction * far + i - 1, h * tok_half : (h + 1) * tok_half] = value.astype(BF16)
        sum_ring(direction, i, h).start()

    with jax.named_scope("weigh_2"):
        weigh(far - 1)
    send_sum(0, 2, 1, False)
    send_sum(1, 2, 0, False)
    send_sum(0, 2, 0, True)
    send_sum(1, 2, 1, True)

    @pl.loop(3, far + 1)
    def _(i):
        with jax.named_scope("weigh"):
            weigh(far + 1 - i)
        with jax.named_scope("sum"):
            for h in range(2):
                for direction in range(2):
                    send_sum(direction, i, 1 - h if direction == 0 else h, True)

    with jax.named_scope("final"):
        for k in range(1, n_tp):
            share_back(k).wait_recv()
        total = stream_ref[...].astype(F32) + own[...]
        for d in range(n_tp):
            total = total + sgot[d].astype(F32)
        own[...] = total
        for h in range(2):
            piece = slice(h * tok_half, (h + 1) * tok_half)
            for direction in range(2):
                sum_ring(direction, far, h).wait_recv()
            result[piece, :] = (
                own[piece, :] + rs_in[0, far - 1, piece].astype(F32) + rs_in[1, far - 1, piece].astype(F32)
            ).astype(BF16)

    @pl.loop(1, far)
    def _(s):
        for h in range(2):
            ring(0, s, h).wait_send()
            ring(1, s, h).wait_send()
        across(0, s).wait_send()
        across(1, s).wait_send()

    ring(0, far, 0).wait_send()
    ring(1, far, 1).wait_send()
    across(0, 0).wait_send()
    across(0, far).wait_send()
    for h in range(n_part):
        for k in range(1, n_tp):
            share(k, h).wait_send()

    @pl.loop(2, far + 1)
    def _(i):
        for h in range(2):
            for d in range(2):
                sum_ring(d, i, h).wait_send()

    sum_ring(0, 1, 0).wait_send()
    sum_ring(1, 1, 1).wait_send()
    for k in range(1, n_tp):
        share_tokens(k).wait_send()
        share_back(k).wait_send()

        @pl.loop(1, far + 1)
        def _(g):
            dispatch(g, k).wait_send()
            give_back(g, k).wait_send()

        @pl.when(c == lax.rem(t + k, n_tp) // 2)
        def _():
            @pl.loop(0, n_own)
            def _(p):
                for m in range(3):
                    weight_copy(m, part_own(p), k).wait_send()

    @pl.when(holder)
    def _():
        for m in range(3):
            weight_to_mate(m).wait_send()

            @pl.loop(0, n_q)
            def _(q):
                for k in range(1, n_tp):
                    weight_on(m, q, k).wait_send()

            if paired:
                @pl.loop(0, n_own)
                def _(p):
                    for k in range(1, n_tp):
                        weight_over(m, part_own(p), k).wait_send()

    @pl.loop(1, far + 1)
    def _(s):
        meta_ring(0, s).wait_send()

    @pl.loop(1, far)
    def _(s):
        meta_ring(1, s).wait_send()


def layer(
    residual_in, q_small, k_small, v_small, q_large, k_large, v_large, gain_qs, gain_ks, gain_ql, gain_kl,
    w_out_small, w_out_large, g_ffn, routes, route_w, w_gate, w_up, w_down, ws_gate, ws_up, ws_down,
):
    n_sp, n_tp = lax.axis_size("sp"), lax.axis_size("tp")
    chips = n_sp // 2
    paired = lax.axis_size("grp") % 2 == 0
    far = chips // 2
    rows = q_small.shape[0]
    rows_total = n_sp * rows // GRID_W
    tok, width = residual_in.shape
    groups = q_small.shape[1] // 64 + q_large.shape[1] // LANES
    slots = max(2, 2 * tok * TOPK // (w_gate.shape[0] * n_sp))
    assert w_gate.shape[0] * 2 == n_tp and 2 * tok == LANES and slots == 8
    (rc_s, rs_s), (cc_s, cs_s) = angle_tables(64, rows_total)
    (rc_l, rs_l), (cc_l, cs_l) = angle_tables(128, rows_total)
    row_tab = jnp.asarray(np.concatenate([rc_s, rs_s, rc_l, rs_l], axis=1)[:, None, :])
    col_tab = jnp.asarray(np.concatenate([cc_s, cs_s, cc_l, cs_l], axis=1))
    operands = [
        q_small, k_small.T, v_small.T, q_large, k_large, v_large, gain_qs.reshape(1, -1), gain_ks.reshape(1, -1),
        gain_ql.reshape(1, -1), gain_kl.reshape(1, -1), g_ffn.reshape(1, -1), row_tab, col_tab, w_out_small, w_out_large,
        residual_in, routes.T, route_w.T, w_gate, w_up, w_down, ws_gate, ws_up, ws_down,
    ]
    n_q = 8
    dma = pltpu.SemaphoreType.DMA
    copies = [pltpu.VMEM(x.shape, x.dtype) for x in operands[:18] + operands[21:]]

    def bf(*shape):
        return pltpu.VMEM(shape, BF16)

    def f32(*shape):
        return pltpu.VMEM(shape, F32)

    moved_rows = (far, n_tp, 2 * slots, width)
    return pl.pallas_call(
        functools.partial(layer_kernel, chips, n_tp, paired),
        out_shape=jax.ShapeDtypeStruct((tok, width), BF16),
        in_specs=[pl.BlockSpec(memory_space=pl.ANY)] * len(operands),
        out_specs=pl.BlockSpec(memory_space=pltpu.VMEM),
        scratch_shapes=copies + [
            bf(groups, rows, LANES), bf(n_sp, rows, 3 * LANES), f32(groups, rows, LANES), f32(groups, rows, LANES),
            f32(groups, rows, LANES), bf(rows, q_small.shape[1] + q_large.shape[1]),
            bf(n_tp, tok, width), bf(n_tp, tok, width),
            bf(tok, width), f32(chips, 16, LANES), bf(chips, tok, width),
            bf(n_tp, *w_gate.shape[1:]), bf(n_tp, *w_up.shape[1:]), bf(n_tp, *w_down.shape[1:]),
            bf(*moved_rows), bf(*moved_rows), bf(*moved_rows), bf(*moved_rows), bf(2, far, tok, width),
            bf(n_tp, tok, width), bf(n_tp, tok, width), bf(n_tp, tok, width),
            f32(n_tp * tok, width), f32(tok, width), f32(2 * tok, width),
            dma((len(copies),)),
            dma((2, far + 1, 2)), dma((2, far + 1, 2)), dma((2, far + 1)), dma((2, far + 1)), dma((4, n_tp)), dma((4, n_tp)),
            dma((2, far + 1)), dma((2, far + 1)), dma((2, far + 1, 4)), dma((2, far + 1, 4)),
            dma((far + 1, n_tp)), dma((far + 1, n_tp)), dma((far + 1, n_tp)), dma((far + 1, n_tp)),
            dma((2, far + 1, 2)), dma((2, far + 1, 2)), dma((n_tp,)), dma((n_tp,)), dma((n_tp,)), dma((n_tp,)),
            *[dma((3, n_q, n_tp))] * 6, dma((3,)),
        ],
        compiler_params=pltpu.CompilerParams(collective_id=0, has_side_effects=True, vmem_limit_bytes=67_043_328),
        name="layer",
    )(*operands)


def solution(mesh):
    part = P(("grp", "sp"), "tp")
    each = P(("grp", "sp", "tp"), None)
    placed = (
        each, part, part, part, part, part, part, P(), P(), P(), P(), P("tp", None), P("tp", None), P(), each, each,
        P("sp", None, "tp"), P("sp", None, "tp"), P("sp", "tp", None), P(None, "tp"), P(None, "tp"), P("tp", None),
    )
    return jax.shard_map(layer, mesh=mesh, in_specs=placed, out_specs=each, check_vma=False)
```

```python
import functools
import math

import jax
import jax.numpy as jnp
import numpy as np
from jax import lax
from jax.experimental import pallas as pl
from jax.experimental.pallas import tpu as pltpu
from jax.sharding import PartitionSpec as P

GRID_W = 64
TOPK = 4
norm_eps = 1e-06
rope_base = 10000.0
far_below = -1e30
LANES = 128
LOG2E = math.log2(math.e)
MESH = pl.DeviceIdType.MESH
F32 = jnp.float32
BF16 = jnp.bfloat16


def angle_tables(channels, rows_total):
    quarter = channels // 4
    lane = np.arange(LANES) % channels
    by_row = lane < channels // 2
    front = lane % (channels // 2) < quarter
    inverse = (1.0 / rope_base ** (np.arange(quarter, dtype=np.float32) / np.float32(quarter))).astype(np.float32)
    freq = inverse[lane % quarter]

    def tables(count, mask):
        angle = np.arange(count, dtype=np.float32)[:, None] * freq[None, :]
        angle = angle.astype(np.float32).astype(np.float64)
        cosine = np.where(mask[None, :], np.cos(angle), 0.0)
        sine = np.where(mask[None, :], np.where(front[None, :], -np.sin(angle), np.sin(angle)), 0.0)
        return cosine.astype(np.float32), sine.astype(np.float32)

    return tables(rows_total, by_row), tables(GRID_W, ~by_row)


def layer_kernel(
    chips, n_tp, paired,
    q_s_in, kt_in, vt_in, q_l_in, k_l_in, v_l_in, g_qs_in, g_ks_in, g_ql_in, g_kl_in, g_ffn_in, row_in, col_in,
    w_s_in, w_l_in, resid_in, routes_in, route_w_in, w_gate, w_up, w_down, ws_gate_in, ws_up_in, ws_down_in,
    result,
    q_s, kt, vt, q_l, k_l, v_l, g_qs, g_ks, g_ql, g_kl, g_ffn, row_tab, col_tab, w_s, w_l, resid, routes, route_w,
    ws_gate, ws_up, ws_down,
    q_all, kv, m_ref, l_ref, acc, heads, part, got,
    stream_ref, meta, tok, wg, wu, wd, sel, rows_in, outs, res, rs_in, stok, spart, sgot, big, own, cbuf,
    load, rs, rr, ds, dr, xs, xr,
    ms, mr, ts, tr, gs, gr, es, er, bs, br, ss, sr, ps, pr, wsnd, wrcv, fs, fr, ys, yr, wl,
):
    me = lax.axis_index("sp")
    t = lax.axis_index("tp")
    z = me // 2
    c = me % 2
    rows = q_s.shape[0]
    half = rows // 2
    far = chips // 2
    n_tok = resid.shape[0]
    n_small = q_s.shape[1] // 64
    n_large = q_l.shape[1] // LANES

    def at(zz):
        return lax.rem(zz + 2 * chips, chips) * 2 + c

    right, left, mate = at(z + 1), at(z - 1), z * 2 + (1 - c)

    pairs = [
        (kt_in, kt), (vt_in, vt), (k_l_in, k_l), (v_l_in, v_l), (g_ks_in, g_ks), (g_kl_in, g_kl), (row_in, row_tab),
        (col_in, col_tab), (q_s_in, q_s), (q_l_in, q_l), (g_qs_in, g_qs), (g_ql_in, g_ql), (routes_in, routes),
        (route_w_in, route_w), (g_ffn_in, g_ffn), (resid_in, resid), (w_s_in, w_s), (w_l_in, w_l),
        (ws_gate_in, ws_gate), (ws_up_in, ws_up), (ws_down_in, ws_down),
    ]
    loads = [pltpu.make_async_copy(src, dst, load.at[i]) for i, (src, dst) in enumerate(pairs)]
    for one in loads[:16]:
        one.start()
    barrier = pltpu.get_barrier_semaphore()
    for peer in (right, left, mate):
        pl.semaphore_signal(barrier, inc=1, device_id={"sp": peer}, device_id_type=MESH)
    for k in range(1, n_tp):
        pl.semaphore_signal(barrier, inc=1, device_id={"tp": lax.rem(t + k, n_tp)}, device_id_type=MESH)

    odd = lax.rem(lax.axis_index("grp"), 2) if paired else 0
    friend = lax.axis_index("grp") + 1 - 2 * odd
    if paired:
        pl.semaphore_signal(barrier, inc=1, device_id={"grp": friend}, device_id_type=MESH)

    with jax.named_scope("load_a"):
        for one in loads[:8]:
            one.wait()
    lane = lax.broadcasted_iota(jnp.int32, (rows, LANES), 1)
    low = lane < 64
    grid_rows = rows // GRID_W
    first = me * grid_rows

    def table(j):
        pieces = []
        for g in range(grid_rows):
            r = row_tab[first + g][:, j * LANES : (j + 1) * LANES]
            pieces.append(col_tab[:, j * LANES : (j + 1) * LANES] + r)
        return jnp.concatenate(pieces, axis=0)

    def turn(x, j, shift):
        front = lax.rem(lane, 2 * shift) < shift
        other = jnp.where(front, pltpu.roll(x, LANES - shift, 1), pltpu.roll(x, shift, 1))
        return x * table(j) + other * table(j + 1)

    def norm_small(x, gain):
        sq = x * x
        lo = jnp.sum(jnp.where(low, sq, 0.0), axis=1, keepdims=True)
        hi = jnp.sum(jnp.where(low, 0.0, sq), axis=1, keepdims=True)
        scale = jnp.where(low, lax.rsqrt(lo / 64 + norm_eps), lax.rsqrt(hi / 64 + norm_eps))
        return x * scale * gain

    def norm_large(x, gain):
        return x * lax.rsqrt(jnp.mean(x * x, axis=1, keepdims=True) + norm_eps) * gain

    def twice(g):
        return jnp.concatenate([g[...], g[...]], axis=1)

    pair = jnp.concatenate([kt[...].astype(F32).T, vt[...].astype(F32).T], axis=1)
    turned = turn(norm_small(pair, twice(g_ks)), 0, 16)
    kv[me, :, 0:LANES] = jnp.where(low, turned, pair).astype(BF16)
    kv[me, :, LANES : 2 * LANES] = turn(norm_large(k_l[...].astype(F32), g_kl[...]), 2, 32).astype(BF16)
    kv[me, :, 2 * LANES : 3 * LANES] = v_l[...]
    with jax.named_scope("entry"):
        pl.semaphore_wait(barrier, 2 + n_tp + paired)

    def ring(direction, s, h):
        sign = 1 - 2 * direction
        block = at(z - sign * (s - 1))
        span = kv.at[block, pl.ds(h * half, half)]
        return pltpu.make_async_remote_copy(
            src_ref=span, dst_ref=span, send_sem=rs.at[direction, s, h], recv_sem=rr.at[direction, s, h],
            device_id={"sp": right if direction == 0 else left}, device_id_type=MESH,
        )

    def across(direction, s):
        sign = 1 - 2 * direction
        block = at(z - sign * s)
        return pltpu.make_async_remote_copy(
            src_ref=kv.at[block], dst_ref=kv.at[block], send_sem=ds.at[direction, s], recv_sem=dr.at[direction, s],
            device_id={"sp": mate}, device_id_type=MESH,
        )

    for h in range(2):
        ring(0, 1, h).start()
        ring(1, 1, h).start()
    across(0, 0).start()

    holder = c == t // 2
    n_q = 8
    moved = [(w_gate, wg, w_gate.shape[1] // n_q), (w_up, wu, w_up.shape[1] // n_q), (w_down, wd, w_down.shape[1] // n_q)]

    def weight_copy(m, q, k):
        src, dst, span = moved[m]
        aim = lax.rem(t + k, n_tp)
        piece = pl.ds(q * span, span)
        return pltpu.make_async_remote_copy(
            src_ref=src.at[lax.rem(aim, 2), piece], dst_ref=dst.at[t, piece], send_sem=wsnd.at[m, q, k],
            recv_sem=wrcv.at[m, q, k], device_id={"tp": aim}, device_id_type=MESH,
        )

    def weight_in(m, q, k):
        src, dst, span = moved[m]
        piece = pl.ds(q * span, span)
        home = dst.at[lax.rem(t + n_tp - k, n_tp), piece]
        return pltpu.make_async_remote_copy(
            src_ref=home, dst_ref=home, send_sem=wsnd.at[m, q, k],
            recv_sem=wrcv.at[m, q, k], device_id={"tp": lax.rem(t + k, n_tp)}, device_id_type=MESH,
        )

    def weight_on(m, q, k):
        src, dst, span = moved[m]
        piece = pl.ds(q * span, span)
        home = dst.at[lax.rem(t + n_tp - k, n_tp), piece]
        return pltpu.make_async_remote_copy(
            src_ref=home, dst_ref=home, send_sem=fs.at[m, q, k], recv_sem=fr.at[m, q, k],
            device_id={"sp": mate}, device_id_type=MESH,
        )

    def weight_mine(m):
        src, dst, _ = moved[m]
        return pltpu.make_async_copy(src.at[lax.rem(t, 2)], dst.at[t], wl.at[m])

    def weight_to_mate(m):
        src, dst, _ = moved[m]
        return pltpu.make_async_remote_copy(
            src_ref=src.at[lax.rem(t, 2)], dst_ref=dst.at[t], send_sem=fs.at[m, 0, 0], recv_sem=fr.at[m, 0, 0],
            device_id={"sp": mate}, device_id_type=MESH,
        )

    def weight_over(m, q, k):
        src, dst, span = moved[m]
        home = dst.at[lax.rem(t + n_tp - k, n_tp), pl.ds(q * span, span)]
        return pltpu.make_async_remote_copy(
            src_ref=home, dst_ref=home, send_sem=ys.at[m, q, k], recv_sem=yr.at[m, q, k],
            device_id={"grp": friend}, device_id_type=MESH,
        )

    n_own = n_q // 2 if paired else n_q

    def part_own(p):
        return 2 * p + odd if paired else p

    def carry_weights(p):
        q = part_own(p)
        for k in range(1, n_tp):
            @pl.when(c == lax.rem(t + k, n_tp) // 2)
            def _():
                for m in range(3):
                    weight_copy(m, q, k).start()

    def relay_weights(p):
        q = part_own(p)

        @pl.when(holder)
        def _():
            for m in range(3):
                for k in range(1, n_tp):
                    weight_in(m, q, k).wait_recv()
                    weight_on(m, q, k).start()
                    if paired:
                        weight_over(m, q, k).start()

    def relay_other(p):
        q = 2 * p + 1 - odd

        @pl.when(holder)
        def _():
            for m in range(3):
                for k in range(1, n_tp):
                    weight_over(m, q, k).wait_recv()
                    weight_on(m, q, k).start()

    def start_late_loads():
        for one in loads[16:]:
            one.start()

        @pl.when(holder)
        def _():
            for m in range(3):
                weight_mine(m).start()
                weight_to_mate(m).start()

    carry_weights(0)
    carry_weights(1)
    with jax.named_scope("load_b"):
        for one in loads[8:14]:
            one.wait()

    slots = result.shape[0] // 8
    experts = n_tp * chips
    ex = lax.broadcasted_iota(jnp.int32, (experts, n_tok), 0)
    hits = [ex == routes[j : j + 1, :] for j in range(TOPK)]
    named = hits[0]
    for one in hits[1:]:
        named = named | one
    before = lax.broadcasted_iota(jnp.int32, (n_tok, n_tok), 0) < lax.broadcasted_iota(jnp.int32, (n_tok, n_tok), 1)
    ahead = jnp.dot(
        jnp.where(named, 1.0, 0.0).astype(BF16), jnp.where(before, 1.0, 0.0).astype(BF16), preferred_element_type=F32
    )
    meta[z] = jnp.zeros(meta.shape[1:], F32)
    for j in range(TOPK):
        place = jnp.sum(jnp.where(hits[j], ahead, 0.0), axis=0, keepdims=True)
        code = routes[j : j + 1, :].astype(F32) * slots + place
        meta[z, j : j + 1, :] = jnp.concatenate([code, code], axis=1)
    meta[z, 8 : 8 + TOPK, :] = jnp.concatenate([route_w[...], route_w[...]], axis=1)

    for p in range(n_small // 2):
        x = q_s[:, p * LANES : (p + 1) * LANES].astype(F32)
        y = turn(norm_small(x, twice(g_qs)), 0, 16)
        q_all[2 * p] = jnp.where(low, y, 0.0).astype(BF16)
        q_all[2 * p + 1] = jnp.where(low, pltpu.roll(y, 64, 1), 0.0).astype(BF16)
    for p in range(n_large):
        x = q_l[:, p * LANES : (p + 1) * LANES].astype(F32)
        q_all[n_small + p] = turn(norm_large(x, g_ql[...]), 2, 32).astype(BF16)
    m_ref[...] = jnp.full_like(m_ref, far_below)
    l_ref[...] = jnp.zeros_like(l_ref)
    acc[...] = jnp.zeros_like(acc)

    def meta_ring(direction, s):
        sign = 1 - 2 * direction
        block = lax.rem(z - sign * (s - 1) + 2 * chips, chips)
        return pltpu.make_async_remote_copy(
            src_ref=meta.at[block], dst_ref=meta.at[block], send_sem=ms.at[direction, s], recv_sem=mr.at[direction, s],
            device_id={"sp": right if direction == 0 else left}, device_id_type=MESH,
        )

    meta_ring(0, 1).start()
    meta_ring(1, 1).start()

    def absorb(blocks):
        def score(g):
            k_at = 0 if g < n_small else LANES
            keys = jnp.concatenate([kv[b, :, k_at : k_at + LANES] for b in blocks], axis=0)
            return lax.dot_general(q_all[g], keys, (((1,), (1,)), ((), ())), preferred_element_type=F32)

        def mix(g, scores):
            v_at = 0 if g < n_small else 2 * LANES
            factor = (64 if g < n_small else 128) ** -0.5 * LOG2E
            pieces = [scores[:, n : n + LANES] for n in range(0, scores.shape[1], LANES)]
            top = functools.reduce(jnp.maximum, pieces)
            old = m_ref[g]
            new = jnp.maximum(old, jnp.max(top, axis=1, keepdims=True))
            shrink = jnp.exp2((old - new) * factor)
            pieces = [jnp.exp2((one - new) * factor) for one in pieces]
            total = functools.reduce(jnp.add, pieces)
            weights = jnp.concatenate([one.astype(BF16) for one in pieces], axis=1)
            values = jnp.concatenate([kv[b, :, v_at : v_at + LANES] for b in blocks], axis=0)
            m_ref[g] = new
            l_ref[g] = l_ref[g] * shrink + total
            acc[g] = acc[g] * shrink + jnp.dot(weights, values, preferred_element_type=F32)

        ready = score(0)
        for g in range(n_small + n_large):
            scores = ready
            if g + 1 < n_small + n_large:
                ready = score(g + 1)
            mix(g, scores)

    def pass_on(s, h):
        ring(0, s, h).wait_recv()
        ring(0, s + 1, h).start()
        ring(1, s, h).wait_recv()
        ring(1, s + 1, h).start()

    def move(s):
        with jax.named_scope("kv_move"):
            for h in range(2):
                @pl.when(s < far - 1)
                def _():
                    pass_on(s, h)

            @pl.when(s == far - 1)
            def _():
                ring(0, s, 0).wait_recv()
                ring(0, far, 0).start()
                ring(1, s, 0).wait_recv()
                ring(0, s, 1).wait_recv()
                ring(1, s, 1).wait_recv()
                ring(1, far, 1).start()

            @pl.when(s == far)
            def _():
                ring(0, far, 0).wait_recv()
                ring(1, far, 1).wait_recv()

            across(0, s).start()
            meta_ring(0, s).wait_recv()

            @pl.when(s < far)
            def _():
                across(1, s).start()
                meta_ring(1, s).wait_recv()
                meta_ring(0, s + 1).start()

            @pl.when(s < far - 1)
            def _():
                meta_ring(1, s + 1).start()

            @pl.when(s == 2)
            def _():
                start_late_loads()

            for p, when in ((2, 3), (3, 5)):
                @pl.when(s == when)
                def _():
                    carry_weights(p)

            for p, when in ((0, far // 2), (1, far - 2), (2, far)):
                @pl.when(s == when)
                def _():
                    relay_weights(p)


    def other(b):
        return b + 1 - 2 * c

    across(0, 0).wait_recv()

    @pl.loop(0, 2)
    def _(s):
        @pl.when(s == 1)
        def _():
            move(1)

        with jax.named_scope("kv_absorb"):
            absorb([at(z - s), jnp.where(s == 0, other(me), at(z + s))])

    @pl.loop(2, far + 1)
    def _(s):
        move(s)
        across(0, s - 1).wait_recv()
        across(1, s - 1).wait_recv()

        @pl.when(s == far)
        def _():
            across(0, far).wait_recv()

        a, b = at(z - s), at(z + s)
        with jax.named_scope("kv_absorb"):
            absorb([a, jnp.where(s == far, other(a), b), other(at(z - s + 1)), other(at(z + s - 1))])

    with jax.named_scope("load_c"):
        for one in loads[14:18]:
            one.wait()

    def finished(g):
        return acc[g] / jnp.sum(l_ref[g], axis=1, keepdims=True)

    for p in range(n_small // 2):
        both = jnp.where(low, pltpu.roll(finished(2 * p), 64, 1), finished(2 * p + 1))
        heads[:, p * LANES : (p + 1) * LANES] = both.astype(BF16)
    for p in range(n_large):
        heads[:, (n_small // 2 + p) * LANES : (n_small // 2 + p + 1) * LANES] = finished(n_small + p).astype(BF16)

    width = resid.shape[1]
    n_cut = 4
    cut = width // n_cut
    split = n_small * 64

    tok_half = n_tok // 2
    n_part = 4
    tok_part = n_tok // n_part

    def share(k, h):
        piece = pl.ds(h * tok_part, tok_part)
        return pltpu.make_async_remote_copy(
            src_ref=part.at[lax.rem(t + k, n_tp), piece], dst_ref=got.at[k, piece], send_sem=xs.at[h, k], recv_sem=xr.at[h, k],
            device_id={"tp": lax.rem(t + k, n_tp)}, device_id_type=MESH,
        )

    with jax.named_scope("project"):
        for n in range(n_cut):
            cols = slice(n * cut, (n + 1) * cut)
            whole = jnp.dot(heads[:, :split], w_s[:, cols], preferred_element_type=F32)
            whole = whole + jnp.dot(heads[:, split:], w_l[:, cols], preferred_element_type=F32)
            for d in range(n_tp):
                part[d, :, cols] = whole[d * n_tok : (d + 1) * n_tok].astype(BF16)
    for h in range(n_part):
        for k in (2, 1, 3):
            share(k, h).start()
    relay_weights(3)

    def share_tokens(k):
        return pltpu.make_async_remote_copy(
            src_ref=stok.at[t], dst_ref=stok.at[t], send_sem=ss.at[k], recv_sem=sr.at[k],
            device_id={"tp": lax.rem(t + k, n_tp)}, device_id_type=MESH,
        )

    def share_back(k):
        return pltpu.make_async_remote_copy(
            src_ref=spart.at[lax.rem(t + k, n_tp)], dst_ref=sgot.at[t], send_sem=ps.at[k], recv_sem=pr.at[k],
            device_id={"tp": lax.rem(t + k, n_tp)}, device_id_type=MESH,
        )

    def zmod(v):
        return lax.rem(v + 2 * chips, chips)

    def token_ring(direction, s, h):
        sign = 1 - 2 * direction
        span = tok.at[zmod(z - sign * (s - 1)), pl.ds(h * tok_part, tok_part)]
        return pltpu.make_async_remote_copy(
            src_ref=span, dst_ref=span, send_sem=ts.at[direction, s, h], recv_sem=tr.at[direction, s, h],
            device_id={"sp": right if direction == 0 else left}, device_id_type=MESH,
        )

    for h in range(n_part):
        with jax.named_scope("head_sum"):
            piece = slice(h * tok_part, (h + 1) * tok_part)
            total = part[t, piece].astype(F32)
            for k in range(1, n_tp):
                share(k, h).wait_recv()
                total = total + got[k, piece].astype(F32)
            stream = (resid[piece, :].astype(F32) + total).astype(BF16)
            stream_ref[piece, :] = stream
            wide = stream.astype(F32)
            scale = lax.rsqrt(jnp.sum(wide * wide, axis=1, keepdims=True) / width + norm_eps)
            tok[z, piece] = (wide * scale * g_ffn[...]).astype(BF16)
            for direction in range(2):
                token_ring(direction, 1, h).start()
    for p in range(4, n_own):
        carry_weights(p)
    stok[t] = tok[z]
    for k in (2, 1, 3):
        share_tokens(k).start()

    wide_lane = lax.broadcasted_iota(jnp.int32, (8 * slots, LANES), 1)
    wide_row = lax.broadcasted_iota(jnp.int32, (8 * slots, LANES), 0)
    second_token = wide_lane // n_tok
    second_row = lax.rem(wide_row // slots, 2)
    code_row = (z * n_tp + wide_row // (2 * slots)) * slots + lax.rem(wide_row, slots)
    code_row = jnp.where(second_token == second_row, code_row, -1).astype(F32)

    def blocks_of(g):
        last = g == far
        return jnp.where(last, z, zmod(z - g)), zmod(z + g)

    def codes(g):
        a, b = blocks_of(g)
        return jnp.where(lax.broadcasted_iota(jnp.int32, meta.shape[1:], 1) < n_tok, meta[a], meta[b])

    def dispatch(g, k):
        return pltpu.make_async_remote_copy(
            src_ref=sel.at[g - 1, lax.rem(t + k, n_tp)], dst_ref=rows_in.at[g - 1, t], send_sem=gs.at[g, k],
            recv_sem=gr.at[g, k], device_id={"tp": lax.rem(t + k, n_tp)}, device_id_type=MESH,
        )

    def give_back(g, k):
        return pltpu.make_async_remote_copy(
            src_ref=outs.at[g - 1, lax.rem(t + k, n_tp)], dst_ref=res.at[g - 1, t], send_sem=es.at[g, k],
            recv_sem=er.at[g, k], device_id={"tp": lax.rem(t + k, n_tp)}, device_id_type=MESH,
        )

    def pick(g):
        a, b = blocks_of(g)
        code = codes(g)
        chosen = jnp.zeros(wide_row.shape, F32)
        for j in range(TOPK):
            chosen = chosen + jnp.where(code[j : j + 1, :] == code_row, 1.0, 0.0)
        chosen = chosen.astype(BF16)
        both = jnp.concatenate([tok[a], tok[b]], axis=0)
        picked = jnp.dot(chosen, both, preferred_element_type=F32).astype(BF16)
        for i in range(n_tp):
            sel[g - 1, i] = picked[i * 2 * slots : (i + 1) * 2 * slots]
        rows_in[g - 1, t] = sel[g - 1, t]
        for k in (2, 1, 3):
            dispatch(g, k).start()

    def takes_far(direction, h):
        return (h < n_part // 2) == (direction == 0)

    def token_step(s):
        for h in range(n_part):
            for d in range(2):
                @pl.when(s < far if not takes_far(d, h) else s <= far)
                def _():
                    token_ring(d, s, h).wait_recv()

                @pl.when(s < far - 1 if not takes_far(d, h) else s < far)
                def _():
                    token_ring(d, s + 1, h).start()

    def weights_in():
        @pl.when(holder)
        def _():
            for m in range(3):
                weight_mine(m).wait()

        @pl.when(jnp.logical_not(holder))
        def _():
            for m in range(3):
                weight_to_mate(m).wait_recv()

                @pl.loop(0, n_q)
                def _(q):
                    for k in range(1, n_tp):
                        weight_on(m, q, k).wait_recv()

    pair_rows = n_tp * 2 * slots

    def expert(first, send=False):
        with jax.named_scope("rows_wait"):
            for n in range(2):
                for k in range(1, n_tp):
                    dispatch(first + n, k).wait_recv()
        with jax.named_scope("expert"):
            x = rows_in[pl.ds(first - 1, 2)].reshape(2 * pair_rows, width)
            big[0 : 2 * pair_rows, :] = jnp.zeros((2 * pair_rows, width), F32)

            @pl.loop(0, n_tp)
            def _(j):
                gate = jnp.dot(x, wg[j], preferred_element_type=F32)
                up = jnp.dot(x, wu[j], preferred_element_type=F32)
                hidden = (gate / (1.0 + jnp.exp(-gate)) * up).astype(BF16)
                big[0 : 2 * pair_rows, :] += jnp.dot(hidden, wd[j], preferred_element_type=F32)

            for n in (1, 0):
                for i in range(n_tp):
                    at_row = n * pair_rows + i * 2 * slots
                    outs[first + n - 1, i] = big[at_row : at_row + 2 * slots, :].astype(BF16)
                if send:
                    return_rows(first + n)
                res[first + n - 1, t] = outs[first + n - 1, t]

    def return_rows(*groups):
        for g in groups:
            for k in (2, 1, 3):
                give_back(g, k).start()

    @pl.loop(1, far + 1)
    def _(s):
        with jax.named_scope("tok_move"):
            token_step(s)
        with jax.named_scope("pick"):
            pick(s)
        with jax.named_scope("relay"):
            if paired:
                for when, these in ((1, range(3)), (3, (3,))):
                    @pl.when(s == when)
                    def _():
                        for p in these:
                            relay_other(p)
            else:
                @pl.when(s == 4)
                def _():
                    for p in range(4, n_own):
                        relay_weights(p)

        @pl.when(s == 4)
        def _():
            with jax.named_scope("shared"):
                for one in loads[18:]:
                    one.wait()
                for k in range(1, n_tp):
                    share_tokens(k).wait_recv()
                x = stok[...].reshape(n_tp * n_tok, width)
                gate = jnp.dot(x, ws_gate[...], preferred_element_type=F32)
                up = jnp.dot(x, ws_up[...], preferred_element_type=F32)
                hidden = (gate / (1.0 + jnp.exp(-gate)) * up).astype(BF16)
                big[...] = jnp.dot(hidden, ws_down[...], preferred_element_type=F32)
                for d in range(n_tp):
                    spart[d] = big[d * n_tok : (d + 1) * n_tok, :].astype(BF16)
                sgot[t] = spart[t]

        @pl.when(s == far - 3)
        def _():
            with jax.named_scope("weights_in"):
                weights_in()

        @pl.when((s >= far - 3) & (s != far - 1))
        def _():
            expert(jnp.where(s == far, far - 3, 2 * (s - (far - 3)) + 1))

    expert(far - 1, send=True)
    return_rows(*range(far - 2, 2, -1))
    for k in (2, 1, 3):
        share_back(k).start()
    return_rows(2, 1)

    @pl.loop(1, far)
    def _(s):
        for h in range(n_part):
            token_ring(0, s, h).wait_send()
            token_ring(1, s, h).wait_send()

    for h in range(n_part):
        token_ring(0 if takes_far(0, h) else 1, far, h).wait_send()

    def sum_ring(direction, i, h):
        piece = pl.ds(h * tok_half, tok_half)
        return pltpu.make_async_remote_copy(
            src_ref=tok.at[direction * far + i - 1, piece], dst_ref=rs_in.at[direction, i - 1, piece],
            send_sem=bs.at[direction, i, h], recv_sem=br.at[direction, i, h],
            device_id={"sp": right if direction == 0 else left}, device_id_type=MESH,
        )

    def weigh(g):
        for k in range(1, n_tp):
            give_back(g, k).wait_recv()
        code = codes(g)
        weight = jnp.zeros(wide_row.shape, F32)
        for j in range(TOPK):
            weight = weight + jnp.where(code[j : j + 1, :] == code_row, code[8 + j : 9 + j, :], 0.0)
        high = weight.astype(BF16)
        rest = weight - high.astype(F32)
        across_rows = jnp.concatenate([high.astype(F32), rest], axis=0).T.astype(BF16)
        back = res[g - 1].reshape(n_tp * 2 * slots, width)
        cbuf[...] = jnp.dot(across_rows, jnp.concatenate([back, back], axis=0), preferred_element_type=F32)

    with jax.named_scope("weigh_first"):
        weigh(far)
    own[...] = cbuf[0:n_tok, :]
    tok[0, 0:tok_half] = cbuf[n_tok : n_tok + tok_half, :].astype(BF16)
    tok[far, tok_half : 2 * tok_half] = cbuf[n_tok + tok_half : 2 * n_tok, :].astype(BF16)
    sum_ring(0, 1, 0).start()
    sum_ring(1, 1, 1).start()

    def send_sum(direction, i, h, add):
        begin = (1 - direction) * n_tok + h * tok_half
        value = cbuf[begin : begin + tok_half, :]
        if add:
            sum_ring(direction, i - 1, h).wait_recv()
            value = value + rs_in[direction, i - 2, h * tok_half : (h + 1) * tok_half].astype(F32)
        tok[direction * far + i - 1, h * tok_half : (h + 1) * tok_half] = value.astype(BF16)
        sum_ring(direction, i, h).start()

    with jax.named_scope("weigh_2"):
        weigh(far - 1)
    send_sum(0, 2, 1, False)
    send_sum(1, 2, 0, False)
    send_sum(0, 2, 0, True)
    send_sum(1, 2, 1, True)

    @pl.loop(3, far + 1)
    def _(i):
        with jax.named_scope("weigh"):
            weigh(far + 1 - i)
        with jax.named_scope("sum"):
            for h in range(2):
                for direction in range(2):
                    send_sum(direction, i, 1 - h if direction == 0 else h, True)

    with jax.named_scope("final"):
        for k in range(1, n_tp):
            share_back(k).wait_recv()
        total = stream_ref[...].astype(F32) + own[...]
        for d in range(n_tp):
            total = total + sgot[d].astype(F32)
        own[...] = total
        for h in range(2):
            piece = slice(h * tok_half, (h + 1) * tok_half)
            for direction in range(2):
                sum_ring(direction, far, h).wait_recv()
            result[piece, :] = (
                own[piece, :] + rs_in[0, far - 1, piece].astype(F32) + rs_in[1, far - 1, piece].astype(F32)
            ).astype(BF16)

    @pl.loop(1, far)
    def _(s):
        for h in range(2):
            ring(0, s, h).wait_send()
            ring(1, s, h).wait_send()
        across(0, s).wait_send()
        across(1, s).wait_send()

    ring(0, far, 0).wait_send()
    ring(1, far, 1).wait_send()
    across(0, 0).wait_send()
    across(0, far).wait_send()
    for h in range(n_part):
        for k in range(1, n_tp):
            share(k, h).wait_send()

    @pl.loop(2, far + 1)
    def _(i):
        for h in range(2):
            for d in range(2):
                sum_ring(d, i, h).wait_send()

    sum_ring(0, 1, 0).wait_send()
    sum_ring(1, 1, 1).wait_send()
    for k in range(1, n_tp):
        share_tokens(k).wait_send()
        share_back(k).wait_send()

        @pl.loop(1, far + 1)
        def _(g):
            dispatch(g, k).wait_send()
            give_back(g, k).wait_send()

        @pl.when(c == lax.rem(t + k, n_tp) // 2)
        def _():
            @pl.loop(0, n_own)
            def _(p):
                for m in range(3):
                    weight_copy(m, part_own(p), k).wait_send()

    @pl.when(holder)
    def _():
        for m in range(3):
            weight_to_mate(m).wait_send()

            @pl.loop(0, n_q)
            def _(q):
                for k in range(1, n_tp):
                    weight_on(m, q, k).wait_send()

            if paired:
                @pl.loop(0, n_own)
                def _(p):
                    for k in range(1, n_tp):
                        weight_over(m, part_own(p), k).wait_send()

    @pl.loop(1, far + 1)
    def _(s):
        meta_ring(0, s).wait_send()

    @pl.loop(1, far)
    def _(s):
        meta_ring(1, s).wait_send()


def layer(
    residual_in, q_small, k_small, v_small, q_large, k_large, v_large, gain_qs, gain_ks, gain_ql, gain_kl,
    w_out_small, w_out_large, g_ffn, routes, route_w, w_gate, w_up, w_down, ws_gate, ws_up, ws_down,
):
    n_sp, n_tp = lax.axis_size("sp"), lax.axis_size("tp")
    chips = n_sp // 2
    paired = lax.axis_size("grp") % 2 == 0
    far = chips // 2
    rows = q_small.shape[0]
    rows_total = n_sp * rows // GRID_W
    tok, width = residual_in.shape
    groups = q_small.shape[1] // 64 + q_large.shape[1] // LANES
    slots = max(2, 2 * tok * TOPK // (w_gate.shape[0] * n_sp))
    assert w_gate.shape[0] * 2 == n_tp and 2 * tok == LANES and slots == 8
    (rc_s, rs_s), (cc_s, cs_s) = angle_tables(64, rows_total)
    (rc_l, rs_l), (cc_l, cs_l) = angle_tables(128, rows_total)
    row_tab = jnp.asarray(np.concatenate([rc_s, rs_s, rc_l, rs_l], axis=1)[:, None, :])
    col_tab = jnp.asarray(np.concatenate([cc_s, cs_s, cc_l, cs_l], axis=1))
    operands = [
        q_small, k_small.T, v_small.T, q_large, k_large, v_large, gain_qs.reshape(1, -1), gain_ks.reshape(1, -1),
        gain_ql.reshape(1, -1), gain_kl.reshape(1, -1), g_ffn.reshape(1, -1), row_tab, col_tab, w_out_small, w_out_large,
        residual_in, routes.T, route_w.T, w_gate, w_up, w_down, ws_gate, ws_up, ws_down,
    ]
    n_q = 8
    dma = pltpu.SemaphoreType.DMA
    copies = [pltpu.VMEM(x.shape, x.dtype) for x in operands[:18] + operands[21:]]

    def bf(*shape):
        return pltpu.VMEM(shape, BF16)

    def f32(*shape):
        return pltpu.VMEM(shape, F32)

    moved_rows = (far, n_tp, 2 * slots, width)
    return pl.pallas_call(
        functools.partial(layer_kernel, chips, n_tp, paired),
        out_shape=jax.ShapeDtypeStruct((tok, width), BF16),
        in_specs=[pl.BlockSpec(memory_space=pl.ANY)] * len(operands),
        out_specs=pl.BlockSpec(memory_space=pltpu.VMEM),
        scratch_shapes=copies + [
            bf(groups, rows, LANES), bf(n_sp, rows, 3 * LANES), f32(groups, rows, LANES), f32(groups, rows, LANES),
            f32(groups, rows, LANES), bf(rows, q_small.shape[1] + q_large.shape[1]),
            bf(n_tp, tok, width), bf(n_tp, tok, width),
            bf(tok, width), f32(chips, 16, LANES), bf(chips, tok, width),
            bf(n_tp, *w_gate.shape[1:]), bf(n_tp, *w_up.shape[1:]), bf(n_tp, *w_down.shape[1:]),
            bf(*moved_rows), bf(*moved_rows), bf(*moved_rows), bf(*moved_rows), bf(2, far, tok, width),
            bf(n_tp, tok, width), bf(n_tp, tok, width), bf(n_tp, tok, width),
            f32(n_tp * tok, width), f32(tok, width), f32(2 * tok, width),
            dma((len(copies),)),
            dma((2, far + 1, 2)), dma((2, far + 1, 2)), dma((2, far + 1)), dma((2, far + 1)), dma((4, n_tp)), dma((4, n_tp)),
            dma((2, far + 1)), dma((2, far + 1)), dma((2, far + 1, 4)), dma((2, far + 1, 4)),
            dma((far + 1, n_tp)), dma((far + 1, n_tp)), dma((far + 1, n_tp)), dma((far + 1, n_tp)),
            dma((2, far + 1, 2)), dma((2, far + 1, 2)), dma((n_tp,)), dma((n_tp,)), dma((n_tp,)), dma((n_tp,)),
            *[dma((3, n_q, n_tp))] * 6, dma((3,)),
        ],
        compiler_params=pltpu.CompilerParams(collective_id=0, has_side_effects=True, vmem_limit_bytes=67_043_328),
        name="layer",
    )(*operands)


def solution(mesh):
    part = P(("grp", "sp"), "tp")
    each = P(("grp", "sp", "tp"), None)
    placed = (
        each, part, part, part, part, part, part, P(), P(), P(), P(), P("tp", None), P("tp", None), P(), each, each,
        P("sp", None, "tp"), P("sp", None, "tp"), P("sp", "tp", None), P(None, "tp"), P(None, "tp"), P("tp", None),
    )
    return jax.shard_map(layer, mesh=mesh, in_specs=placed, out_specs=each, check_vma=False)
```
